512 devices in a mesh: sp: 64 (over z, y), tp: 8 (over x, core).
Axes of the slice: x: 4, y: 8, z: 8, core: 2. Of those that a mesh axis runs over, the one named last changes fastest.
Arguments:
- tokens: bfloat16 [65536, 2048], P('sp'), may hold values from -6 to 6
- norm_gain: float32 [2048], replicated, may hold values from 0.1 to 1.9
- w_query: bfloat16 [2048, 512], P(None, 'tp'), may hold values from -0.79549513 to 0.79549513
- w_key: bfloat16 [2048, 128], P('sp'), may hold values from -0.79549513 to 0.79549513
- w_value: bfloat16 [2048, 128], P('sp'), may hold values from -0.125 to 0.125
- w_pool_in: bfloat16 [2048, 512], P(None, 'tp'), may hold values from -0.125 to 0.125
- sink_logit: float32 [8], P('tp'), may hold values from 3 to 7
- pool_scale: float32 [512], P('tp'), may hold values from 0.05 to 0.5
- w_out: bfloat16 [1024, 2048], P('tp', 'sp'), may hold values from -0.75 to 0.75
Outputs:
- mixed_out: bfloat16 [65536, 2048], P(('sp', 'tp'))
The draws below stay inside these ranges and needn't reach their ends.
All inputs are finite; a program needn't handle non-finite values.
Results may differ from the reference program's by a relative error of at most 0.03.
The reference program's roundings to bfloat16 on the way (of `normed`, `query`, `key`, `value`, `pool_in`, `weights`, `attended` and `pooled`) count: a program that leaves them out, or rounds other values in their place, can miss the bound.
Values may be sent and summed in bfloat16 or wider, within the bound.
No kernel may reach another device: no remote copies, remote signals or barrier semaphores. Data moves between devices by JAX's collectives and lax.ppermute only.
A program may use at most 64 MiB of HBM per device.

```python
import math
import jax
import jax.numpy as jnp
from jax import lax

D = 2048
HEAD = 64
QH = 8
KVH = 2
POOL_CH = 128
POOL_W = 512
WINDOW = 128
QB = 128
SEQ = 65536


def projection_draw(key, shape):
    values = jax.random.truncated_normal(key, -6.0, 6.0, shape, jnp.float32) * D ** (-0.5)
    return values.astype(jnp.bfloat16)


def draw_w_query(key, part):
    return projection_draw(jax.random.fold_in(key, 11), (D, QH * HEAD))


def draw_w_key(key, part):
    return projection_draw(jax.random.fold_in(key, 23), (D, KVH * HEAD))


def level_of(key, dims, pieces, smallest, top_value):
    level = 1.0
    for dim, parts in pieces:
        steps = jax.random.uniform(jax.random.fold_in(jax.random.fold_in(key, 6), dim), (parts,), jnp.float32, smallest / len(pieces), top_value / len(pieces))
        level = level * jnp.repeat(jnp.exp(steps), dims[dim] // parts).reshape((-1,) + (1,) * (len(dims) - 1 - dim))
    return level


def centred(rng, dims, scale, reach, pieces=(), kind=jnp.bfloat16):
    entries = scale * jax.random.normal(rng, dims, jnp.float32)
    if pieces:
        entries = entries * level_of(rng, dims, pieces, -0.22, 0.18)
    return jnp.clip(entries, -reach, reach).astype(kind)


def setup_inputs(seed: int = 0) -> dict:
    seeds = jax.random.split(jax.random.key(seed), 10)
    tokens = centred(seeds[0], (SEQ, D), 1.0, 6.0, ((0, 64),))
    norm_gain = jnp.clip(1.0 + 0.18 * jax.random.normal(seeds[1], (D,), jnp.float32), 0.1, 1.9)
    w_query = draw_w_query(jax.random.fold_in(seeds[9], 71), 0)
    w_key = draw_w_key(jax.random.fold_in(seeds[9], 71), 0)
    w_value = centred(seeds[4], (D, KVH * HEAD), D ** -0.5, 0.125, ((0, 64),))
    w_pool_in = centred(seeds[5], (D, POOL_W), D ** -0.5, 0.125, ((1, 8),))
    sink_logit = jnp.clip(3.0 + 4.0 * jax.random.uniform(seeds[6], (QH,), jnp.float32) ** level_of(seeds[6], (QH,), ((0, 8),), -0.2, 0.2), 3.0, 7.0)
    pool_scale = jnp.clip(jnp.exp(math.log(0.5) - 2.3025851 * jax.random.uniform(seeds[7], (POOL_W,), jnp.float32) ** level_of(seeds[7], (POOL_W,), ((0, 8),), -0.2, 0.2)), 0.05, 0.5)
    w_out = centred(seeds[8], (QH * HEAD + POOL_W, D), (4.0 * (QH * HEAD + POOL_W) ** -0.5), 0.75, ((0, 8), (1, 64)))
    return {"tokens": tokens, "norm_gain": norm_gain, "w_query": w_query, "w_key": w_key, "w_value": w_value, "w_pool_in": w_pool_in, "sink_logit": sink_logit, "pool_scale": pool_scale, "w_out": w_out}


NEG_BIG = -1e+30
POOL_SPANS = (2, 4, 8, 16)

def layer_normed(tokens, norm_gain):
    values = tokens.astype(jnp.float32)
    center = lax.optimization_barrier(jnp.mean(values, axis=-1, keepdims=True))
    spread = lax.optimization_barrier(jnp.mean(jnp.square(values - center), axis=-1, keepdims=True))
    return ((values - center) * lax.rsqrt(spread + 1e-06) * norm_gain).astype(jnp.bfloat16)

def rotate(values, positions):
    half = HEAD // 2
    inverse = 10000.0 ** (-jnp.arange(half, dtype=jnp.float32) / half)
    angles = positions[:, None] * inverse[None, :]
    cosine = jnp.cos(angles)[:, None, :]
    sine = jnp.sin(angles)[:, None, :]
    first = values[..., :half]
    second = values[..., half:]
    return jnp.concatenate([first * cosine - second * sine, first * sine + second * cosine], axis=-1)

def reference(tokens, norm_gain, w_query, w_key, w_value, w_pool_in, sink_logit, pool_scale, w_out):
    length = tokens.shape[0]
    group = QH // KVH
    normed = layer_normed(tokens, norm_gain)
    positions = jnp.arange(length).astype(jnp.float32)
    query = rotate(jnp.dot(normed, w_query, preferred_element_type=jnp.float32).reshape(length, QH, HEAD), positions).astype(jnp.bfloat16)
    key = rotate(jnp.dot(normed, w_key, preferred_element_type=jnp.float32).reshape(length, KVH, HEAD), positions).astype(jnp.bfloat16)
    value = jnp.dot(normed, w_value, preferred_element_type=jnp.float32).astype(jnp.bfloat16).reshape(length, KVH, HEAD)
    pool_in = jnp.dot(normed, w_pool_in, preferred_element_type=jnp.float32).astype(jnp.bfloat16)
    key_padded = jnp.pad(key, ((WINDOW, WINDOW), (0, 0), (0, 0)))
    value_padded = jnp.pad(value, ((WINDOW, WINDOW), (0, 0), (0, 0)))
    span = QB + 2 * WINDOW
    sink_grid = sink_logit.reshape(KVH, group)[:, :, None, None]

    def attend(start):
        queries = lax.dynamic_slice_in_dim(query, start, QB, 0).reshape(QB, KVH, group, HEAD)
        keys = lax.dynamic_slice_in_dim(key_padded, start, span, 0)
        values = lax.dynamic_slice_in_dim(value_padded, start, span, 0)
        scores = jnp.einsum('ikgd,jkd->kgij', queries.astype(jnp.float32), keys.astype(jnp.float32)) * HEAD ** (-0.5)
        query_pos = start + jnp.arange(QB).astype(jnp.int32)
        key_pos = start - WINDOW + jnp.arange(span).astype(jnp.int32)
        valid = (jnp.abs(query_pos[:, None] - key_pos[None, :]) <= WINDOW) & (key_pos[None, :] >= 0) & (key_pos[None, :] < length)
        scores = jnp.where(valid, scores, NEG_BIG)
        highest = jnp.maximum(lax.optimization_barrier(jnp.max(scores, axis=-1, keepdims=True)), sink_grid)
        expo = jnp.where(valid, jnp.exp(scores - highest), 0.0)
        total = lax.optimization_barrier(jnp.sum(expo, axis=-1, keepdims=True)) + jnp.exp(sink_grid - highest)
        weights = (expo / total).astype(jnp.bfloat16)
        result = jnp.einsum('kgij,jkd->ikgd', weights.astype(jnp.float32), values.astype(jnp.float32))
        return result.reshape(QB, QH * HEAD).astype(jnp.bfloat16)
    starts = (jnp.arange(length // QB) * QB).astype(jnp.int32)
    attended = lax.map(attend, starts).reshape(length, QH * HEAD)
    pool_vals = pool_in.astype(jnp.float32)
    running = jnp.pad(jnp.cumsum(pool_vals, axis=0), ((1, 0), (0, 0)))
    where_at = jnp.arange(length).astype(jnp.int32)
    means = []
    for index, width in enumerate(POOL_SPANS):
        lower = jnp.clip(where_at - width // 2, 0, length)
        upper = jnp.clip(where_at + width // 2, 0, length)
        block = running[:, index * POOL_CH:(index + 1) * POOL_CH]
        means.append((block[upper] - block[lower]) / (upper - lower).astype(jnp.float32)[:, None])
    pooled = ((jnp.concatenate(means, axis=1) - pool_vals) * pool_scale).astype(jnp.bfloat16)
    joined = jnp.concatenate([attended, pooled], axis=1)
    return jnp.dot(joined, w_out, preferred_element_type=jnp.float32).astype(jnp.bfloat16)
```

```python
import jax
import jax.numpy as jnp
from jax import lax
from jax.sharding import Mesh
from jax.sharding import PartitionSpec as P

HEAD = 64
QH = 8
KVH = 2
POOL_CH = 128
WINDOW = 128
QB = 128


NEG_BIG = -1e30
POOL_SPANS = (2, 4, 8, 16)
SP = ("z", "y")
TP = ("x", "c")


def extended(block, sides, width):
    for axis, dim in sides:
        count = lax.axis_size(axis)
        forward = [(i, i + 1) for i in range(count - 1)]
        backward = [(target, source) for source, target in forward]
        low = lax.ppermute(
            lax.slice_in_dim(block, block.shape[dim] - width, None, axis=dim), axis, forward
        )
        high = lax.ppermute(lax.slice_in_dim(block, 0, width, axis=dim), axis, backward)
        block = jnp.concatenate([low, block, high], axis=dim)
    return block


def from_everyone(x, axis):
    peers = lax.axis_size(axis)
    return lax.all_to_all(jnp.broadcast_to(x[None], (peers, *x.shape)), axis, 0, 0, tiled=True)


def layer_normed(tokens, norm_gain):
    values = tokens.astype(jnp.float32)
    center = jnp.mean(values, axis=-1, keepdims=True)
    spread = jnp.mean(jnp.square(values - center), axis=-1, keepdims=True)
    return ((values - center) * lax.rsqrt(spread + 1e-06) * norm_gain).astype(jnp.bfloat16)


def rotate(values, positions):
    half = HEAD // 2
    inverse = 10000.0 ** (-jnp.arange(half, dtype=jnp.float32) / half)
    angles = positions[:, None] * inverse[None, :]
    cosine = jnp.cos(angles)[:, None, :]
    sine = jnp.sin(angles)[:, None, :]
    first = values[..., :half]
    second = values[..., half:]
    return jnp.concatenate(
        [first * cosine - second * sine, first * sine + second * cosine], axis=-1
    )


def swapped(piece):
    side = lax.axis_size("z")
    place = lambda z, y, t: (z * side + y) * side + t
    pairs = [
        (place(z, y, t), place(t, y, z))
        for z in range(side)
        for y in range(side)
        for t in range(side)
    ]
    return lax.ppermute(piece, ("z", "y", "x", "c"), pairs)


def body(tokens, norm_gain, w_query, w_key, w_value, w_pool_in, sink_logit, pool_scale, w_out):
    local_rows = tokens.shape[0]
    seq_total = local_rows * lax.axis_size(SP)
    offset = lax.axis_index(SP) * local_rows
    tp_place = lax.axis_index(TP)
    local_heads = w_query.shape[1] // HEAD
    local_pool = w_pool_in.shape[1]
    reach = POOL_SPANS[-1] // 2
    normed = layer_normed(tokens, norm_gain)
    positions = (offset + jnp.arange(local_rows)).astype(jnp.float32)
    query = rotate(
        jnp.dot(normed, w_query, preferred_element_type=jnp.float32).reshape(
            local_rows, local_heads, HEAD
        ),
        positions,
    ).astype(jnp.bfloat16)
    key_head = tp_place * local_heads // (QH // KVH)
    key_cols = lax.dynamic_slice_in_dim(w_key, key_head * HEAD, HEAD, 1)
    value_cols = lax.dynamic_slice_in_dim(w_value, key_head * HEAD, HEAD, 1)
    out_piece = swapped(w_out.T)
    both = jnp.concatenate([jnp.concatenate([key_cols, value_cols], axis=1), out_piece], axis=0)
    weights_all = from_everyone(both, SP)
    kv_cols = weights_all[:, : key_cols.shape[0]].reshape(-1, 2 * HEAD)
    out_cols = weights_all[:, key_cols.shape[0] :].reshape(lax.axis_size("z"), -1, w_out.shape[0])
    kv_sum = jnp.dot(normed, kv_cols, preferred_element_type=jnp.float32)
    key_sum, value_sum = kv_sum[:, :HEAD], kv_sum[:, HEAD:]
    key = rotate(key_sum[:, None, :], positions)[:, 0, :].astype(jnp.bfloat16)
    value = value_sum.astype(jnp.bfloat16)
    key_value = jnp.concatenate([key, value], axis=1)
    pool_in = jnp.dot(normed, w_pool_in, preferred_element_type=jnp.float32).astype(jnp.bfloat16)
    widened = extended(jnp.concatenate([key_value, pool_in], axis=1), ((SP, 0),), WINDOW)
    kv_wide = widened[:, : 2 * HEAD]
    pool_wide = widened[WINDOW - reach : WINDOW + local_rows + reach, 2 * HEAD :]
    span = QB + 2 * WINDOW
    sink_here = sink_logit[:, None, None]
    results = []
    for block in range(local_rows // QB):
        queries = query[block * QB : (block + 1) * QB]
        keys = kv_wide[block * QB : block * QB + span, :HEAD]
        values = kv_wide[block * QB : block * QB + span, HEAD:]
        scores = jnp.einsum(
            "ihd,jd->hij", queries, keys, preferred_element_type=jnp.float32
        ) * HEAD ** (-0.5)
        query_pos = offset + block * QB + jnp.arange(QB)
        key_pos = offset + block * QB - WINDOW + jnp.arange(span)
        valid = (
            (jnp.abs(query_pos[:, None] - key_pos[None, :]) <= WINDOW)
            & (key_pos[None, :] >= 0)
            & (key_pos[None, :] < seq_total)
        )
        scores = jnp.where(valid, scores, NEG_BIG)
        highest = jnp.maximum(jnp.max(scores, axis=-1, keepdims=True), sink_here)
        expo = jnp.where(valid, jnp.exp(scores - highest), 0.0)
        total = jnp.sum(expo, axis=-1, keepdims=True) + jnp.exp(sink_here - highest)
        weights = (expo / total).astype(jnp.bfloat16)
        result = jnp.einsum("hij,jd->ihd", weights, values, preferred_element_type=jnp.float32)
        results.append(result.reshape(QB, local_heads * HEAD).astype(jnp.bfloat16))
    attended = jnp.concatenate(results, axis=0)
    pool_vals = pool_wide.astype(jnp.float32)
    window_sum = pool_vals
    global_pos = offset + jnp.arange(local_rows)
    channel = tp_place * local_pool + jnp.arange(local_pool)
    window_group = channel // POOL_CH
    measured = jnp.zeros((local_rows, local_pool), jnp.float32)
    stride = 1
    for index, width in enumerate(POOL_SPANS):
        window_sum = window_sum[:-stride] + window_sum[stride:]
        stride = width
        sums = window_sum[reach - width // 2 : reach - width // 2 + local_rows]
        counted = (
            jnp.minimum(global_pos + width // 2, seq_total)
            - jnp.maximum(global_pos - width // 2, 0)
        ).astype(jnp.float32)
        measured = measured + jnp.where(
            window_group[None, :] == index, sums / counted[:, None], 0.0
        )
    pooled = ((measured - pool_vals[reach : reach + local_rows]) * pool_scale).astype(jnp.bfloat16)
    local = jnp.concatenate([attended, pooled], axis=1)
    joined_all = from_everyone(local, TP)
    count = joined_all.shape[0]
    halves = out_cols.reshape(2, count // 2, -1, 2, HEAD)
    matched = jnp.moveaxis(halves, 3, 2).reshape(2, count, -1, HEAD)
    matched = jnp.concatenate([matched[0], matched[1]], axis=2)
    partial_cols = jnp.einsum(
        "ptc,pnc->tn", joined_all, matched, preferred_element_type=jnp.float32
    ).astype(jnp.bfloat16)
    return lax.all_to_all(partial_cols, TP, split_axis=0, concat_axis=1, tiled=True)


def solution(mesh):
    mesh = Mesh(mesh.devices.reshape(8, 8, 4, 2), SP + TP)
    in_specs = (
        P(SP, None),
        P(),
        P(None, TP),
        P(SP, None),
        P(SP, None),
        P(None, TP),
        P(TP),
        P(TP),
        P(TP, SP),
    )
    out_specs = P(SP + TP, None)
    return jax.shard_map(body, mesh=mesh, in_specs=in_specs, out_specs=out_specs, check_vma=False)
```

```python
import functools

import jax
import jax.numpy as jnp
from jax import lax
from jax.experimental import pallas as pl
from jax.experimental.pallas import tpu as pltpu
from jax.sharding import Mesh
from jax.sharding import PartitionSpec as P

HEAD = 64
WINDOW = 128
QB = 128
LANES = 128
ROWS = 256
EDGE = 16
POOL_SPANS = (2, 4, 8, 16)
NEG_BIG = -1e30
SP = ("z", "y")
TP = ("x", "c")
INTERPRET = False


def from_everyone(x, axis):
    peers = lax.axis_size(axis)
    return lax.all_to_all(jnp.broadcast_to(x[None], (peers, *x.shape)), axis, 0, 0, tiled=True)


def swapped(piece):
    side, depth = lax.axis_size("z"), lax.axis_size("y")
    place = lambda z, y, t: (z * depth + y) * side + t
    pairs = [
        (place(z, y, t), place(t, y, z))
        for z in range(side)
        for y in range(depth)
        for t in range(side)
    ]
    return lax.ppermute(piece, SP + TP, pairs)


def three_parts(x):
    high = lax.reduce_precision(x, 8, 7)
    middle = lax.reduce_precision(x - high, 8, 7)
    low = x - high - middle
    return jnp.stack([high, middle, low]).astype(jnp.bfloat16)


def rope_tables(offset, rows):
    half = HEAD // 2
    inverse = 10000.0 ** (-jnp.arange(half, dtype=jnp.float32) / half)
    positions = (offset + jnp.arange(rows)).astype(jnp.float32)
    angles = positions[:, None] * inverse[None, :]
    cosine, sine = jnp.cos(angles), jnp.sin(angles)
    return (
        jnp.concatenate([cosine] * 4, axis=1),
        jnp.concatenate([-sine, sine, -sine, sine], axis=1),
    )


def project(tokens, gain, qp, ex, cosine, sine, q_out, kv_out, pool_out, weights):
    @pl.when(pl.program_id(0) == 0)
    def _():
        depth = weights.shape[0]
        weights[:, :LANES] = qp[0, :depth]
        weights[:, LANES : 2 * LANES] = qp[1, :depth]
        weights[:, 2 * LANES :] = ex[:, : ex.shape[1] // 2].reshape(depth, LANES)

    values = tokens[...].astype(jnp.float32)
    center = jnp.mean(values, axis=-1, keepdims=True)
    values = values - center
    spread = jnp.mean(values * values, axis=-1, keepdims=True)
    normed = (values * lax.rsqrt(spread + 1e-06) * gain[...]).astype(jnp.bfloat16)
    sums = jnp.dot(normed, weights[...], preferred_element_type=jnp.float32)
    query = jnp.concatenate([sums[:, :HEAD], sums[:, 2 * HEAD : 3 * HEAD]], axis=1)
    pool = jnp.concatenate([sums[:, HEAD : 2 * HEAD], sums[:, 3 * HEAD : 4 * HEAD]], axis=1)
    kv = sums[:, 4 * HEAD :]
    lane = lax.broadcasted_iota(jnp.int32, (ROWS, LANES), 1)
    first = lane % HEAD < HEAD // 2

    def turned(x):
        other = jnp.where(first, pltpu.roll(x, LANES - HEAD // 2, 1), pltpu.roll(x, HEAD // 2, 1))
        return x * cosine[...] + other * sine[...]

    q_out[...] = (turned(query) * HEAD ** (-0.5)).astype(jnp.bfloat16)
    kv_out[...] = jnp.where(lane < HEAD, turned(kv), kv).astype(jnp.bfloat16)
    pool_out[...] = pool.astype(jnp.bfloat16)


def mix(blocks_total, place, sink, scale, q, kv, pool, halo, out, kv_wide, pool_wide):
    core, first_block, group = place[0], place[1], place[2]
    rows = q.shape[0]
    kv_wide[pl.ds(pl.multiple_of((1 - core) * QB, QB), rows), :] = kv[...]
    kv_wide[pl.ds(pl.multiple_of(core * rows, QB), QB), :] = halo[:QB, :]
    edge = halo[QB:, :].astype(jnp.float32)
    pool_wide[:EDGE, :] = edge
    pool_wide[EDGE : EDGE + rows, :] = pool[...].astype(jnp.float32)
    pool_wide[EDGE + rows :, :] = edge
    lane = lax.broadcasted_iota(jnp.int32, (QB, LANES), 1)
    row = lax.broadcasted_iota(jnp.int32, (2 * QB, 3 * QB), 0) % QB
    column = lax.broadcasted_iota(jnp.int32, (2 * QB, 3 * QB), 1)
    near = (column >= row) & (column <= row + 2 * WINDOW)
    upper = lax.broadcasted_iota(jnp.int32, (2 * QB, 1), 0) < QB
    sinks = jnp.where(upper, sink[0], sink[1])
    half = lax.shift_left(1, group)
    for i in range(rows // (2 * QB)):
        start = pl.multiple_of(core * QB + 2 * QB * i, QB)
        block = first_block + core + 2 * i
        pair = q[pl.ds(start, QB), :]
        zero = jnp.zeros_like(pair)
        lower_head = jnp.where(lane < HEAD, pair, zero)
        upper_head = jnp.concatenate([pair[:, HEAD:], zero[:, HEAD:]], axis=1)
        queries = jnp.concatenate([lower_head, upper_head], axis=0)
        keys = kv_wide[2 * QB * i : 2 * QB * i + 3 * QB, :]
        scores = lax.dot_general(
            queries, keys, (((1,), (1,)), ((), ())), preferred_element_type=jnp.float32
        )
        least = jnp.where(block == 0, QB, 0)
        limit = jnp.where(block == blocks_total - 1, 2 * QB, 3 * QB)
        valid = near & (column >= least) & (column < limit)
        scores = jnp.where(valid, scores, NEG_BIG)
        top = jnp.maximum(jnp.max(scores, axis=-1, keepdims=True), sinks)
        expo = jnp.where(valid, jnp.exp(scores - top), 0.0)
        total = jnp.sum(expo, axis=-1, keepdims=True) + jnp.exp(sinks - top)
        weights = (expo / total).astype(jnp.bfloat16)
        mixed = jnp.dot(weights, keys, preferred_element_type=jnp.float32)
        attended = jnp.concatenate([mixed[:QB, HEAD:], mixed[QB:, HEAD:]], axis=1)
        out[i * QB : (i + 1) * QB, :LANES] = attended.astype(jnp.bfloat16)

        near_rows = pool_wide[pl.ds(start, QB + 2 * EDGE), :]
        size = QB + 2 * EDGE
        sums = near_rows + pltpu.roll(near_rows, 1, 0)
        chosen = sums
        for index in range(1, len(POOL_SPANS)):
            step = POOL_SPANS[index] // 4
            sums = pltpu.roll(sums, step, 0) + pltpu.roll(sums, size - step, 0)
            chosen = jnp.where(group == index, sums, chosen)
        position = block * QB + lax.broadcasted_iota(jnp.int32, (QB, 1), 0)
        counted = jnp.minimum(position + half, blocks_total * QB) - jnp.maximum(position - half, 0)
        mean = chosen[EDGE : EDGE + QB] / counted.astype(jnp.float32)
        pooled = (mean - near_rows[EDGE : EDGE + QB]) * scale[...]
        out[i * QB : (i + 1) * QB, LANES:] = pooled.astype(jnp.bfloat16)


def output_product(joined, columns, out):
    peers, width = joined.shape[0], columns.shape[2]
    for side in range(2):
        total = None
        for i in range(peers):
            weights = jnp.concatenate([columns[side, i], columns[side, peers + i]], axis=1)
            part = lax.dot_general(
                joined[i], weights, (((1,), (1,)), ((), ())), preferred_element_type=jnp.float32
            )
            total = part if total is None else total + part
        out[:, side * width : (side + 1) * width] = total.astype(jnp.bfloat16)


def body(tokens, norm_gain, w_query, w_key, w_value, w_pool_in, sink_logit, pool_scale, w_out):
    rows, depth = tokens.shape
    core, chip, sp_place = lax.axis_index("c"), lax.axis_index("x"), lax.axis_index(SP)
    sp_count = lax.axis_size(SP)
    key_head = chip // (lax.axis_size("x") // (w_key.shape[1] // HEAD))
    bf16 = jnp.bfloat16

    out_piece = swapped(w_out.T)

    small = jnp.concatenate(
        [three_parts(pool_scale), jnp.broadcast_to(three_parts(sink_logit), (3, HEAD))], axis=1
    )
    small = jnp.pad(small, ((0, EDGE - 3), (0, 0)))
    own = jnp.concatenate([jnp.concatenate([w_query, w_pool_in], axis=1), small], axis=0)
    chip_weights = from_everyone(own, "c")
    small = jnp.sum(chip_weights[:, depth : depth + 3].astype(jnp.float32), axis=1)
    scale = small[:, :HEAD].reshape(1, LANES)
    sink = small[:, HEAD]

    cosine, sine = rope_tables(sp_place * rows, rows)
    key_cols = lax.dynamic_slice_in_dim(w_key, key_head * HEAD, HEAD, 1)
    value_cols = lax.dynamic_slice_in_dim(w_value, key_head * HEAD, HEAD, 1)
    both = jnp.concatenate([jnp.concatenate([key_cols, value_cols], axis=1), out_piece], axis=0)
    both, cosine, sine, scale, sink = lax.optimization_barrier((both, cosine, sine, scale, sink))
    exchanged = from_everyone(both, SP)

    whole = lambda *shape: pl.BlockSpec(shape, lambda i: (0,) * len(shape))
    part = lambda *shape: pl.BlockSpec(shape, lambda i: (i,) + (0,) * (len(shape) - 1))
    query, kv, pool_in = pl.pallas_call(
        project,
        grid=(rows // ROWS,),
        in_specs=[
            part(ROWS, depth),
            whole(1, depth),
            whole(*chip_weights.shape),
            whole(*exchanged.shape),
            part(ROWS, LANES),
            part(ROWS, LANES),
        ],
        out_specs=[part(ROWS, LANES)] * 3,
        out_shape=[jax.ShapeDtypeStruct((rows, LANES), bf16)] * 3,
        scratch_shapes=[pltpu.VMEM((depth, 3 * LANES), bf16)],
        name="project",
        interpret=INTERPRET,
    )(tokens, norm_gain[None, :], chip_weights, exchanged, cosine, sine)

    tail = jnp.concatenate([kv[rows - QB :], pool_in[rows - EDGE :]], axis=0)
    head = jnp.concatenate([kv[:QB], pool_in[:EDGE]], axis=0)
    pairs = [(2 * s, 2 * s + 2) for s in range(sp_count - 1)]
    pairs += [(2 * s + 3, 2 * s + 1) for s in range(sp_count - 1)]
    halo = lax.ppermute(jnp.where(core == 0, tail, head), SP + ("c",), pairs)

    out_cols = from_everyone(exchanged[:, key_cols.shape[0] :], "c")
    out_cols = out_cols.reshape(2, lax.axis_size("z"), -1, LANES)

    place = jnp.stack([core, sp_place * (rows // QB), chip]).astype(jnp.int32)
    smem = pl.BlockSpec(memory_space=pltpu.SMEM)
    vmem = pl.BlockSpec(memory_space=pltpu.VMEM)
    local = pl.pallas_call(
        functools.partial(mix, sp_count * (rows // QB)),
        in_specs=[smem, smem] + [vmem] * 5,
        out_specs=vmem,
        out_shape=jax.ShapeDtypeStruct((rows // 2, 2 * LANES), bf16),
        scratch_shapes=[
            pltpu.VMEM((rows + QB, LANES), bf16),
            pltpu.VMEM((rows + 2 * EDGE, LANES), jnp.float32),
        ],
        name="mix",
        interpret=INTERPRET,
    )(place, sink, scale, query, kv, pool_in, halo)

    joined = from_everyone(local, "x")
    partial_cols = pl.pallas_call(
        output_product,
        in_specs=[vmem] * 2,
        out_specs=vmem,
        out_shape=jax.ShapeDtypeStruct((rows // 2, 2 * out_cols.shape[2]), bf16),
        name="output_product",
        interpret=INTERPRET,
    )(joined, out_cols)
    return lax.all_to_all(partial_cols, "x", split_axis=0, concat_axis=1, tiled=True)


def solution(mesh):
    devices = mesh.devices
    mesh = Mesh(devices.reshape(8, devices.size // 64, 4, 2), SP + TP)
    in_specs = (
        P(SP, None),
        P(),
        P(None, TP),
        P(SP, None),
        P(SP, None),
        P(None, TP),
        P(TP),
        P(TP),
        P(TP, SP),
    )
    out_specs = P(SP + TP, None)
    return jax.shard_map(body, mesh=mesh, in_specs=in_specs, out_specs=out_specs, check_vma=False)
```

```python
import functools

import jax
import jax.numpy as jnp
from jax import lax
from jax.experimental import pallas as pl
from jax.experimental.pallas import tpu as pltpu
from jax.sharding import Mesh
from jax.sharding import PartitionSpec as P

HEAD = 64
WINDOW = 128
QB = 128
LANES = 128
ROWS = 256
EDGE = 16
POOL_SPANS = (2, 4, 8, 16)
NEG_BIG = -1e30
SP = ("z", "y")
TP = ("x", "c")
INTERPRET = False


def from_everyone(x, axis):
    peers = lax.axis_size(axis)
    return lax.all_to_all(jnp.broadcast_to(x[None], (peers, *x.shape)), axis, 0, 0, tiled=True)


def swapped(piece):
    side, depth = lax.axis_size("z"), lax.axis_size("y")
    place = lambda z, y, t: (z * depth + y) * side + t
    pairs = [
        (place(z, y, t), place(t, y, z))
        for z in range(side)
        for y in range(depth)
        for t in range(side)
    ]
    return lax.ppermute(piece, SP + TP, pairs)


def three_parts(x):
    high = lax.reduce_precision(x, 8, 7)
    middle = lax.reduce_precision(x - high, 8, 7)
    low = x - high - middle
    return jnp.stack([high, middle, low]).astype(jnp.bfloat16)


def rope_tables(offset, rows):
    half = HEAD // 2
    inverse = 10000.0 ** (-jnp.arange(half, dtype=jnp.float32) / half)
    positions = (offset + jnp.arange(rows)).astype(jnp.float32)
    angles = positions[:, None] * inverse[None, :]
    return jnp.cos(angles), jnp.sin(angles)


def project(
    tokens, gain, own, other, ex, cosine, sine, q_out, kv_out, pool_out, send, weights
):
    core = lax.axis_index("c")
    step = pl.program_id(0)
    depth = weights.shape[0]

    @pl.when(step == 0)
    def _():
        weights[:, 2 * LANES :] = ex[...].reshape(depth, LANES)

    for place in range(2):

        @pl.when((step == 0) & (core == place))
        def _():
            weights[:, place * LANES : (place + 1) * LANES] = own[:depth]
            weights[:, (1 - place) * LANES : (2 - place) * LANES] = other[:depth]

    values = tokens[...].astype(jnp.float32)
    center = jnp.mean(values, axis=-1, keepdims=True)
    values = values - center
    spread = jnp.mean(values * values, axis=-1, keepdims=True)
    normed = (values * lax.rsqrt(spread + 1e-06) * gain[...]).astype(jnp.bfloat16)
    sums = jnp.dot(normed, weights[...], preferred_element_type=jnp.float32)
    query = jnp.concatenate([sums[:, :HEAD], sums[:, 2 * HEAD : 3 * HEAD]], axis=1)
    pool = jnp.concatenate([sums[:, HEAD : 2 * HEAD], sums[:, 3 * HEAD : 4 * HEAD]], axis=1)
    kv = sums[:, 4 * HEAD :]
    lane = lax.broadcasted_iota(jnp.int32, (ROWS, LANES), 1)
    first = lane % HEAD < HEAD // 2

    wide_cosine = jnp.concatenate([cosine[...]] * 4, axis=1)
    wide_sine = jnp.concatenate([-sine[...], sine[...]] * 2, axis=1)

    def turned(x):
        other = jnp.where(first, pltpu.roll(x, LANES - HEAD // 2, 1), pltpu.roll(x, HEAD // 2, 1))
        return x * wide_cosine + other * wide_sine

    kv = jnp.where(lane < HEAD, turned(kv), kv).astype(jnp.bfloat16)
    pool = pool.astype(jnp.bfloat16)
    q_out[...] = (turned(query) * HEAD ** (-0.5)).astype(jnp.bfloat16)
    kv_out[...] = kv
    pool_out[...] = pool

    @pl.when((step == 0) & (core == 1))
    def _():
        send[:QB] = kv[:QB]
        send[QB:] = pool[:EDGE]

    @pl.when((step == pl.num_programs(0) - 1) & (core == 0))
    def _():
        send[:QB] = kv[ROWS - QB :]
        send[QB:] = pool[ROWS - EDGE :]


def mix(own, other, q, kv, pool, halo, out, kv_wide, pool_wide):
    core, group = lax.axis_index("c"), lax.axis_index("x")
    rows = q.shape[0]
    blocks_total = lax.axis_size(SP) * (rows // QB)
    first_block = lax.axis_index(SP) * (rows // QB)
    mine = jnp.sum(own[:3].astype(jnp.float32), axis=0, keepdims=True)
    theirs = jnp.sum(other[:3].astype(jnp.float32), axis=0, keepdims=True)
    first = jnp.where(core == 0, mine, theirs)
    second = jnp.where(core == 0, theirs, mine)
    scale = jnp.concatenate([first[:, :HEAD], second[:, :HEAD]], axis=1)
    kv_wide[pl.ds(pl.multiple_of((1 - core) * QB, QB), rows), :] = kv[...]
    kv_wide[pl.ds(pl.multiple_of(core * rows, QB), QB), :] = halo[:QB, :]
    edge = halo[QB:, :].astype(jnp.float32)
    pool_wide[:EDGE, :] = edge
    pool_wide[EDGE : EDGE + rows, :] = pool[...].astype(jnp.float32)
    pool_wide[EDGE + rows :, :] = edge
    lane = lax.broadcasted_iota(jnp.int32, (QB, LANES), 1)
    row = lax.broadcasted_iota(jnp.int32, (2 * QB, 3 * QB), 0) % QB
    column = lax.broadcasted_iota(jnp.int32, (2 * QB, 3 * QB), 1)
    near = (column >= row) & (column <= row + 2 * WINDOW)
    upper = lax.broadcasted_iota(jnp.int32, (2 * QB, 1), 0) < QB
    sinks = jnp.where(upper, first[:, HEAD : HEAD + 1], second[:, HEAD : HEAD + 1])
    half = lax.shift_left(1, group)
    for i in range(rows // (2 * QB)):
        start = pl.multiple_of(core * QB + 2 * QB * i, QB)
        block = first_block + core + 2 * i
        pair = q[pl.ds(start, QB), :]
        zero = jnp.zeros_like(pair)
        lower_head = jnp.where(lane < HEAD, pair, zero)
        upper_head = jnp.concatenate([pair[:, HEAD:], zero[:, HEAD:]], axis=1)
        queries = jnp.concatenate([lower_head, upper_head], axis=0)
        keys = kv_wide[2 * QB * i : 2 * QB * i + 3 * QB, :]
        scores = lax.dot_general(
            queries, keys, (((1,), (1,)), ((), ())), preferred_element_type=jnp.float32
        )
        least = jnp.where(block == 0, QB, 0)
        limit = jnp.where(block == blocks_total - 1, 2 * QB, 3 * QB)
        valid = near & (column >= least) & (column < limit)
        scores = jnp.where(valid, scores, NEG_BIG)
        top = jnp.maximum(jnp.max(scores, axis=-1, keepdims=True), sinks)
        expo = jnp.where(valid, jnp.exp(scores - top), 0.0)
        total = jnp.sum(expo, axis=-1, keepdims=True) + jnp.exp(sinks - top)
        weights = (expo / total).astype(jnp.bfloat16)
        mixed = jnp.dot(weights, keys, preferred_element_type=jnp.float32)
        attended = jnp.concatenate([mixed[:QB, HEAD:], mixed[QB:, HEAD:]], axis=1)

        near_rows = pool_wide[pl.ds(start, QB + 2 * EDGE), :]
        size = QB + 2 * EDGE
        sums = near_rows + pltpu.roll(near_rows, 1, 0)
        chosen = sums
        for index in range(1, len(POOL_SPANS)):
            step = POOL_SPANS[index] // 4
            sums = pltpu.roll(sums, step, 0) + pltpu.roll(sums, size - step, 0)
            chosen = jnp.where(group == index, sums, chosen)
        position = block * QB + lax.broadcasted_iota(jnp.int32, (QB, 1), 0)
        counted = jnp.minimum(position + half, blocks_total * QB) - jnp.maximum(position - half, 0)
        mean = chosen[EDGE : EDGE + QB] / counted.astype(jnp.float32)
        pooled = (mean - near_rows[EDGE : EDGE + QB]) * scale
        both = jnp.concatenate([attended, pooled], axis=1).astype(jnp.bfloat16)
        for peer in range(out.shape[0]):
            out[peer, i * QB : (i + 1) * QB] = both


def output_product(joined, own, other, out):
    core = lax.axis_index("c")
    peers = joined.shape[0]

    def product(columns):
        columns = columns.reshape(2 * peers, -1, LANES)
        total = None
        for i in range(peers):
            weights = jnp.concatenate([columns[i], columns[peers + i]], axis=1)
            part = lax.dot_general(
                joined[i], weights, (((1,), (1,)), ((), ())), preferred_element_type=jnp.float32
            )
            total = part if total is None else total + part
        return total.astype(jnp.bfloat16)

    mine, theirs = product(own[...]), product(other[...])
    out[...] = jnp.concatenate(
        [jnp.where(core == 0, mine, theirs), jnp.where(core == 0, theirs, mine)], axis=1
    )


def body(tokens, norm_gain, w_query, w_key, w_value, w_pool_in, sink_logit, pool_scale, w_out):
    rows, depth = tokens.shape
    sp_count = lax.axis_size(SP)
    bf16 = jnp.bfloat16

    out_piece = swapped(w_out.T)

    small = jnp.concatenate(
        [three_parts(pool_scale), jnp.broadcast_to(three_parts(sink_logit), (3, HEAD))], axis=1
    )
    small = jnp.pad(small, ((0, EDGE - 3), (0, 0)))
    own = jnp.concatenate([jnp.concatenate([w_query, w_pool_in], axis=1), small], axis=0)
    other = lax.ppermute(own, "c", [(0, 1), (1, 0)])

    cosine, sine = rope_tables(lax.axis_index(SP) * rows, rows)
    key_head = lax.axis_index("x") // (lax.axis_size("x") // (w_key.shape[1] // HEAD))
    key_cols = lax.dynamic_slice_in_dim(w_key, key_head * HEAD, HEAD, 1)
    value_cols = lax.dynamic_slice_in_dim(w_value, key_head * HEAD, HEAD, 1)
    both = jnp.concatenate([jnp.concatenate([key_cols, value_cols], axis=1), out_piece], axis=0)
    both, cosine, sine, own, other = lax.optimization_barrier((both, cosine, sine, own, other))
    exchanged = from_everyone(both, SP)
    peers, pieces = exchanged.shape[0], key_cols.shape[0]

    at = lambda *shape: lambda *place: pl.BlockSpec(shape, lambda i: place)
    whole = lambda *shape: pl.BlockSpec(shape, lambda i: (0,) * len(shape))
    part = lambda *shape: pl.BlockSpec(shape, lambda i: (i,) + (0,) * (len(shape) - 1))
    query, kv, pool_in, send = pl.pallas_call(
        project,
        grid=(rows // ROWS,),
        in_specs=[
            part(ROWS, depth),
            whole(1, depth),
            whole(*own.shape),
            whole(*own.shape),
            whole(peers, pieces, LANES),
            part(ROWS, HEAD // 2),
            part(ROWS, HEAD // 2),
        ],
        out_specs=[part(ROWS, LANES)] * 3 + [whole(QB + EDGE, LANES)],
        out_shape=[jax.ShapeDtypeStruct((rows, LANES), bf16)] * 3
        + [jax.ShapeDtypeStruct((QB + EDGE, LANES), bf16)],
        scratch_shapes=[pltpu.VMEM((depth, 3 * LANES), bf16)],
        name="project",
        interpret=INTERPRET,
    )(tokens, norm_gain[None, :], own, other, exchanged, cosine, sine)

    pairs = [(2 * s, 2 * s + 2) for s in range(sp_count - 1)]
    pairs += [(2 * s + 3, 2 * s + 1) for s in range(sp_count - 1)]
    halo = lax.ppermute(send, SP + ("c",), pairs)

    own_cols = exchanged[:, pieces:]
    other_cols = lax.ppermute(own_cols, "c", [(0, 1), (1, 0)])

    peers_x = lax.axis_size("x")
    small_rows = at(EDGE, LANES)(depth // EDGE, 0)
    local = pl.pallas_call(
        mix,
        grid=(1,),
        in_specs=[small_rows, small_rows]
        + [whole(rows, LANES)] * 3
        + [whole(QB + EDGE, LANES)],
        out_specs=whole(peers_x, rows // 2, 2 * LANES),
        out_shape=jax.ShapeDtypeStruct((peers_x, rows // 2, 2 * LANES), bf16),
        scratch_shapes=[
            pltpu.VMEM((rows + QB, LANES), bf16),
            pltpu.VMEM((rows + 2 * EDGE, LANES), jnp.float32),
        ],
        name="mix",
        interpret=INTERPRET,
    )(own, other, query, kv, pool_in, halo)

    local, other_cols, own_cols = lax.optimization_barrier((local, other_cols, own_cols))
    joined = lax.all_to_all(local, "x", 0, 0, tiled=True)
    width = 2 * own_cols.shape[0] // lax.axis_size("z") * own_cols.shape[1]
    partial_cols = pl.pallas_call(
        output_product,
        grid=(peers_x,),
        in_specs=[
            pl.BlockSpec((peers_x, QB, 2 * LANES), lambda i: (0, i, 0)),
            whole(*own_cols.shape),
            whole(*own_cols.shape),
        ],
        out_specs=part(QB, width),
        out_shape=jax.ShapeDtypeStruct((rows // 2, width), bf16),
        name="output_product",
        interpret=INTERPRET,
    )(joined, own_cols, other_cols)
    return lax.all_to_all(partial_cols, "x", split_axis=0, concat_axis=1, tiled=True)


def solution(mesh):
    devices = mesh.devices
    mesh = Mesh(devices.reshape(8, devices.size // 64, 4, 2), SP + TP)
    in_specs = (
        P(SP, None),
        P(),
        P(None, TP),
        P(SP, None),
        P(SP, None),
        P(None, TP),
        P(TP),
        P(TP),
        P(TP, SP),
    )
    out_specs = P(SP + TP, None)
    return jax.shard_map(body, mesh=mesh, in_specs=in_specs, out_specs=out_specs, check_vma=False)
```

```python
import functools

import jax
import jax.numpy as jnp
from jax import lax
from jax.experimental import pallas as pl
from jax.experimental.pallas import tpu as pltpu
from jax.sharding import Mesh
from jax.sharding import PartitionSpec as P

HEAD = 64
WINDOW = 128
QB = 128
LANES = 128
ROWS = 256
EDGE = 16
POOL_SPANS = (2, 4, 8, 16)
NEG_BIG = -1e30
SP = ("z", "y")
TP = ("x", "c")
INTERPRET = False


def from_everyone(x, axis):
    peers = lax.axis_size(axis)
    return lax.all_to_all(jnp.broadcast_to(x[None], (peers, *x.shape)), axis, 0, 0, tiled=True)


def swapped(piece):
    side, depth = lax.axis_size("z"), lax.axis_size("y")
    place = lambda z, y, t: (z * depth + y) * side + t
    pairs = [
        (place(z, y, t), place(t, y, z))
        for z in range(side)
        for y in range(depth)
        for t in range(side)
    ]
    return lax.ppermute(piece, SP + TP, pairs)


def three_parts(x):
    high = lax.reduce_precision(x, 8, 7)
    middle = lax.reduce_precision(x - high, 8, 7)
    low = x - high - middle
    return jnp.concatenate([high, middle, low], axis=0).astype(jnp.bfloat16)


def rope_tables(offset, rows):
    half = HEAD // 2
    inverse = 10000.0 ** (-jnp.arange(half, dtype=jnp.float32) / half)
    positions = (offset + jnp.arange(rows)).astype(jnp.float32)
    angles = positions[None, :] * inverse[:, None]
    return jnp.cos(angles), jnp.sin(angles)


def turned(x, cosine, sine):
    lane = lax.broadcasted_iota(jnp.int32, x.shape, 1)
    wide_cosine = jnp.concatenate([cosine] * 4, axis=0).T
    wide_sine = jnp.concatenate([-sine, sine] * 2, axis=0).T
    half = HEAD // 2
    other = jnp.where(lane % HEAD < half, pltpu.roll(x, LANES - half, 1), pltpu.roll(x, half, 1))
    return x * wide_cosine + other * wide_sine


def project(tokens, gain, own, other, cosine, sine, normed_out, q_out, pool_out, weights):
    core = lax.axis_index("c")
    for place in range(2):

        @pl.when((pl.program_id(0) == 0) & (core == place))
        def _():
            for source, head in ((own, place), (other, 1 - place)):
                weights[head * HEAD : (head + 1) * HEAD] = source[:HEAD]
                weights[LANES + head * HEAD : LANES + (head + 1) * HEAD] = source[HEAD:LANES]

    values = tokens[...].astype(jnp.float32)
    center = jnp.mean(values, axis=-1, keepdims=True)
    values = values - center
    spread = jnp.mean(values * values, axis=-1, keepdims=True)
    normed = (values * lax.rsqrt(spread + 1e-06) * gain[...]).astype(jnp.bfloat16)
    normed_out[...] = normed
    sums = lax.dot_general(
        normed, weights[...], (((1,), (1,)), ((), ())), preferred_element_type=jnp.float32
    )
    query = turned(sums[:, :LANES], cosine[...], sine[...])
    q_out[...] = (query * HEAD ** (-0.5)).astype(jnp.bfloat16)
    pool_out[...] = sums[:, LANES:].astype(jnp.bfloat16)


def project_kv(normed, pool, ex, cosine, sine, kv_out, send):
    core = lax.axis_index("c")
    step = pl.program_id(0)
    rows = normed.shape[0]
    sums = jnp.dot(
        normed[...], ex[...].reshape(-1, LANES), preferred_element_type=jnp.float32
    )
    lane = lax.broadcasted_iota(jnp.int32, sums.shape, 1)
    kv = jnp.where(lane < HEAD, turned(sums, cosine[...], sine[...]), sums).astype(jnp.bfloat16)
    kv_out[...] = kv

    @pl.when((step == 0) & (core == 1))
    def _():
        send[:QB] = kv[:QB]
        send[QB:] = pool[:EDGE]

    @pl.when((step == pl.num_programs(0) - 1) & (core == 0))
    def _():
        send[:QB] = kv[rows - QB :]
        send[QB:] = pool[rows - EDGE :]


def mix(own, other, q, kv, pool, halo, out, kv_wide, pool_wide):
    core, group = lax.axis_index("c"), lax.axis_index("x")
    i = pl.program_id(0)
    rows = q.shape[0]
    blocks_total = lax.axis_size(SP) * (rows // QB)
    first_block = lax.axis_index(SP) * (rows // QB)
    mine = jnp.sum(own[:3, :LANES].astype(jnp.float32), axis=0, keepdims=True)
    theirs = jnp.sum(other[:3, :LANES].astype(jnp.float32), axis=0, keepdims=True)
    first = jnp.where(core == 0, mine, theirs)
    second = jnp.where(core == 0, theirs, mine)
    scale = jnp.concatenate([first[:, :HEAD], second[:, :HEAD]], axis=1)

    @pl.when(i == 0)
    def _():
        kv_wide[pl.ds(pl.multiple_of((1 - core) * QB, QB), rows), :] = kv[...]
        kv_wide[pl.ds(pl.multiple_of(core * rows, QB), QB), :] = halo[:QB, :]
        edge = halo[QB:, :].astype(jnp.float32)
        pool_wide[:EDGE, :] = edge
        pool_wide[EDGE : EDGE + rows, :] = pool[...].astype(jnp.float32)
        pool_wide[EDGE + rows :, :] = edge

    lane = lax.broadcasted_iota(jnp.int32, (QB, LANES), 1)
    row = lax.broadcasted_iota(jnp.int32, (2 * QB, 3 * QB), 0) % QB
    column = lax.broadcasted_iota(jnp.int32, (2 * QB, 3 * QB), 1)
    near = (column >= row) & (column <= row + 2 * WINDOW)
    upper = lax.broadcasted_iota(jnp.int32, (2 * QB, 1), 0) < QB
    sinks = jnp.where(upper, first[:, HEAD : HEAD + 1], second[:, HEAD : HEAD + 1])
    half = lax.shift_left(1, group)
    start = pl.multiple_of(core * QB + 2 * QB * i, QB)
    block = first_block + core + 2 * i
    pair = q[pl.ds(start, QB), :]
    zero = jnp.zeros_like(pair)
    lower_head = jnp.where(lane < HEAD, pair, zero)
    upper_head = jnp.concatenate([pair[:, HEAD:], zero[:, HEAD:]], axis=1)
    queries = jnp.concatenate([lower_head, upper_head], axis=0)
    keys = kv_wide[pl.ds(pl.multiple_of(2 * QB * i, QB), 3 * QB), :]
    scores = lax.dot_general(
        queries, keys, (((1,), (1,)), ((), ())), preferred_element_type=jnp.float32
    )
    least = jnp.where(block == 0, QB, 0)
    limit = jnp.where(block == blocks_total - 1, 2 * QB, 3 * QB)
    valid = near & (column >= least) & (column < limit)
    scores = jnp.where(valid, scores, NEG_BIG)
    top = jnp.maximum(jnp.max(scores, axis=-1, keepdims=True), sinks)
    expo = jnp.where(valid, jnp.exp(scores - top), 0.0)
    total = jnp.sum(expo, axis=-1, keepdims=True) + jnp.exp(sinks - top)
    weights = (expo / total).astype(jnp.bfloat16)
    mixed = jnp.dot(weights, keys, preferred_element_type=jnp.float32)
    attended = jnp.concatenate([mixed[:QB, HEAD:], mixed[QB:, HEAD:]], axis=1)

    near_rows = pool_wide[pl.ds(start, QB + 2 * EDGE), :]
    size = QB + 2 * EDGE
    sums = near_rows + pltpu.roll(near_rows, 1, 0)
    chosen = sums
    for index in range(1, len(POOL_SPANS)):
        step = POOL_SPANS[index] // 4
        sums = pltpu.roll(sums, step, 0) + pltpu.roll(sums, size - step, 0)
        chosen = jnp.where(group == index, sums, chosen)
    position = block * QB + lax.broadcasted_iota(jnp.int32, (QB, 1), 0)
    counted = jnp.minimum(position + half, blocks_total * QB) - jnp.maximum(position - half, 0)
    mean = chosen[EDGE : EDGE + QB] / counted.astype(jnp.float32)
    pooled = (mean - near_rows[EDGE : EDGE + QB]) * scale
    both = jnp.concatenate([attended, pooled], axis=1).astype(jnp.bfloat16)
    for peer in range(out.shape[0]):
        out[peer] = both


def output_product(joined, own, other, out):
    core = lax.axis_index("c")
    peers = joined.shape[0]

    def product(columns):
        columns = columns.reshape(2 * peers, -1, LANES)
        total = None
        for i in range(peers):
            weights = jnp.concatenate([columns[i], columns[peers + i]], axis=1)
            part = lax.dot_general(
                joined[i], weights, (((1,), (1,)), ((), ())), preferred_element_type=jnp.float32
            )
            total = part if total is None else total + part
        return total.astype(jnp.bfloat16)

    mine, theirs = product(own[...]), product(other[...])
    out[...] = jnp.concatenate(
        [jnp.where(core == 0, mine, theirs), jnp.where(core == 0, theirs, mine)], axis=1
    )


def body(tokens, norm_gain, w_query, w_key, w_value, w_pool_in, sink_logit, pool_scale, w_out):
    rows, depth = tokens.shape
    sp_count = lax.axis_size(SP)
    bf16 = jnp.bfloat16

    out_piece = swapped(w_out.T)

    small = jnp.concatenate([pool_scale, jnp.broadcast_to(sink_logit, (HEAD,))])[None, :]
    small = three_parts(lax.optimization_barrier(small))
    small = jnp.pad(small, ((0, EDGE - 3), (0, depth - LANES)))
    own = jnp.concatenate([w_query.T, w_pool_in.T, small], axis=0)
    other = lax.ppermute(own, "c", [(0, 1), (1, 0)])

    cosine, sine = rope_tables(lax.axis_index(SP) * rows, rows)
    key_head = lax.axis_index("x") // (lax.axis_size("x") // (w_key.shape[1] // HEAD))
    key_cols = lax.dynamic_slice_in_dim(w_key, key_head * HEAD, HEAD, 1)
    value_cols = lax.dynamic_slice_in_dim(w_value, key_head * HEAD, HEAD, 1)
    both = jnp.concatenate([jnp.concatenate([key_cols, value_cols], axis=1), out_piece], axis=0)
    exchanged = from_everyone(both, SP)
    peers, pieces = exchanged.shape[0], key_cols.shape[0]

    at = lambda *shape: lambda *place: pl.BlockSpec(shape, lambda i: place)
    whole = lambda *shape: pl.BlockSpec(shape, lambda i: (0,) * len(shape))
    part = lambda *shape: pl.BlockSpec(shape, lambda i: (i,) + (0,) * (len(shape) - 1))
    along = lambda *shape: pl.BlockSpec(shape, lambda i: (0, i))
    shaped = lambda *shape: jax.ShapeDtypeStruct(shape, bf16)
    tables = [along(HEAD // 2, ROWS)] * 2
    normed, query, pool_in = pl.pallas_call(
        project,
        grid=(rows // ROWS,),
        in_specs=[part(ROWS, depth), whole(1, depth)] + [whole(*own.shape)] * 2 + tables,
        out_specs=[part(ROWS, depth), part(ROWS, LANES), part(ROWS, LANES)],
        out_shape=[shaped(rows, depth), shaped(rows, LANES), shaped(rows, LANES)],
        scratch_shapes=[pltpu.VMEM((2 * LANES, depth), bf16)],
        name="project",
        interpret=INTERPRET,
    )(tokens, norm_gain[None, :], own, other, cosine, sine)
    kv, send = pl.pallas_call(
        project_kv,
        grid=(rows // ROWS,),
        in_specs=[part(ROWS, depth), part(ROWS, LANES), whole(peers, pieces, LANES)] + tables,
        out_specs=[part(ROWS, LANES), whole(QB + EDGE, LANES)],
        out_shape=[shaped(rows, LANES), shaped(QB + EDGE, LANES)],
        name="project_kv",
        interpret=INTERPRET,
    )(normed, pool_in, exchanged, cosine, sine)

    pairs = [(2 * s, 2 * s + 2) for s in range(sp_count - 1)]
    pairs += [(2 * s + 3, 2 * s + 1) for s in range(sp_count - 1)]
    exchanged, send = lax.optimization_barrier((exchanged, send))
    halo = lax.ppermute(send, SP + ("c",), pairs)
    other_exchanged = lax.ppermute(exchanged, "c", [(0, 1), (1, 0)])

    peers_x = lax.axis_size("x")
    small_rows = at(EDGE, depth)(LANES // EDGE, 0)
    local = pl.pallas_call(
        mix,
        grid=(peers_x,),
        in_specs=[small_rows, small_rows]
        + [whole(rows, LANES)] * 3
        + [whole(QB + EDGE, LANES)],
        out_specs=pl.BlockSpec((peers_x, QB, 2 * LANES), lambda i: (0, i, 0)),
        out_shape=shaped(peers_x, rows // 2, 2 * LANES),
        scratch_shapes=[
            pltpu.VMEM((rows + QB, LANES), bf16),
            pltpu.VMEM((rows + 2 * EDGE, LANES), jnp.float32),
        ],
        name="mix",
        interpret=INTERPRET,
    )(own, other, query, kv, pool_in, halo)

    local, other_exchanged = lax.optimization_barrier((local, other_exchanged))
    joined = lax.all_to_all(local, "x", 0, 0, tiled=True)
    columns = at(peers, pieces, LANES)(0, 1, 0)
    width = 2 * peers // lax.axis_size("z") * pieces
    partial_cols = pl.pallas_call(
        output_product,
        grid=(1,),
        in_specs=[whole(*joined.shape), columns, columns],
        out_specs=whole(rows // 2, width),
        out_shape=shaped(rows // 2, width),
        name="output_product",
        interpret=INTERPRET,
    )(joined, exchanged, other_exchanged)
    return lax.all_to_all(partial_cols, "x", split_axis=0, concat_axis=1, tiled=True)


def solution(mesh):
    devices = mesh.devices
    mesh = Mesh(devices.reshape(8, devices.size // 64, 4, 2), SP + TP)
    in_specs = (
        P(SP, None),
        P(),
        P(None, TP),
        P(SP, None),
        P(SP, None),
        P(None, TP),
        P(TP),
        P(TP),
        P(TP, SP),
    )
    out_specs = P(SP + TP, None)
    return jax.shard_map(body, mesh=mesh, in_specs=in_specs, out_specs=out_specs, check_vma=False)
```

```python
import jax
import jax.numpy as jnp
from jax import lax
from jax.experimental import pallas as pl
from jax.experimental.pallas import tpu as pltpu
from jax.sharding import Mesh
from jax.sharding import PartitionSpec as P

HEAD = 64
WINDOW = 128
QB = 128
LANES = 128
ROWS = 256
EDGE = 16
POOL_SPANS = (2, 4, 8, 16)
NEG_BIG = -1e30
SP = ("z", "y")
TP = ("x", "c")
INTERPRET = False


def from_everyone(x, axis):
    peers = lax.axis_size(axis)
    return lax.all_to_all(jnp.broadcast_to(x[None], (peers, *x.shape)), axis, 0, 0, tiled=True)


def swapped(piece):
    side, depth = lax.axis_size("z"), lax.axis_size("y")
    place = lambda z, y, t: (z * depth + y) * side + t
    pairs = [
        (place(z, y, t), place(t, y, z))
        for z in range(side)
        for y in range(depth)
        for t in range(side)
    ]
    return lax.ppermute(piece, SP + TP, pairs)


def three_parts(x):
    high = lax.reduce_precision(x, 8, 7)
    middle = lax.reduce_precision(x - high, 8, 7)
    low = x - high - middle
    return jnp.concatenate([high, middle, low], axis=0).astype(jnp.bfloat16)


def rope_tables(offset, rows):
    half = HEAD // 2
    inverse = 10000.0 ** (-jnp.arange(half, dtype=jnp.float32) / half)
    positions = (offset + jnp.arange(rows)).astype(jnp.float32)
    angles = positions[None, :] * inverse[:, None]
    return jnp.cos(angles), jnp.sin(angles)


def turned(x, cosine, sine):
    lane = lax.broadcasted_iota(jnp.int32, x.shape, 1)
    wide_cosine = jnp.concatenate([cosine] * 4, axis=0).T
    wide_sine = jnp.concatenate([-sine, sine] * 2, axis=0).T
    half = HEAD // 2
    other = jnp.where(lane % HEAD < half, pltpu.roll(x, LANES - half, 1), pltpu.roll(x, half, 1))
    return x * wide_cosine + other * wide_sine


def project(tokens, gain, own, other, cosine, sine, normed_out, q_out, pool_out, weights):
    core = lax.axis_index("c")
    for place in range(2):

        @pl.when((pl.program_id(0) == 0) & (core == place))
        def _():
            for source, head in ((own, place), (other, 1 - place)):
                weights[head * HEAD : (head + 1) * HEAD] = source[:HEAD]
                weights[LANES + head * HEAD : LANES + (head + 1) * HEAD] = source[HEAD:LANES]

    values = tokens[...].astype(jnp.float32)
    center = jnp.mean(values, axis=-1, keepdims=True)
    values = values - center
    spread = jnp.mean(values * values, axis=-1, keepdims=True)
    normed = (values * lax.rsqrt(spread + 1e-06) * gain[...]).astype(jnp.bfloat16)
    normed_out[...] = normed
    sums = lax.dot_general(
        normed, weights[...], (((1,), (1,)), ((), ())), preferred_element_type=jnp.float32
    )
    query = turned(sums[:, :LANES], cosine[...], sine[...])
    q_out[...] = (query * HEAD ** (-0.5)).astype(jnp.bfloat16)
    pool_out[...] = sums[:, LANES:].astype(jnp.bfloat16)


def project_kv(normed, pool, ex, cosine, sine, kv_out, send):
    core = lax.axis_index("c")
    step = pl.program_id(0)
    rows = normed.shape[0]
    sums = jnp.dot(
        normed[...], ex[...].reshape(-1, LANES), preferred_element_type=jnp.float32
    )
    lane = lax.broadcasted_iota(jnp.int32, sums.shape, 1)
    kv = jnp.where(lane < HEAD, turned(sums, cosine[...], sine[...]), sums).astype(jnp.bfloat16)
    kv_out[...] = kv

    @pl.when((step == 0) & (core == 1))
    def _():
        send[:QB] = kv[:QB]
        send[QB:] = pool[:EDGE]

    @pl.when((step == pl.num_programs(0) - 1) & (core == 0))
    def _():
        send[:QB] = kv[rows - QB :]
        send[QB:] = pool[rows - EDGE :]


def mix(own, other, q, kv, pool, halo, out, kv_wide, pool_wide):
    core, group = lax.axis_index("c"), lax.axis_index("x")
    i = pl.program_id(0)
    rows = q.shape[0]
    blocks_total = lax.axis_size(SP) * (rows // QB)
    first_block = lax.axis_index(SP) * (rows // QB)
    mine = jnp.sum(own[:3, :LANES].astype(jnp.float32), axis=0, keepdims=True)
    theirs = jnp.sum(other[:3, :LANES].astype(jnp.float32), axis=0, keepdims=True)
    first = jnp.where(core == 0, mine, theirs)
    second = jnp.where(core == 0, theirs, mine)
    scale = jnp.concatenate([first[:, :HEAD], second[:, :HEAD]], axis=1)

    @pl.when(i == 0)
    def _():
        kv_wide[pl.ds(pl.multiple_of((1 - core) * QB, QB), rows), :] = kv[...]
        kv_wide[pl.ds(pl.multiple_of(core * rows, QB), QB), :] = halo[:QB, :]
        edge = halo[QB:, :].astype(jnp.float32)
        pool_wide[:EDGE, :] = edge
        pool_wide[EDGE : EDGE + rows, :] = pool[...].astype(jnp.float32)
        pool_wide[EDGE + rows :, :] = edge

    lane = lax.broadcasted_iota(jnp.int32, (QB, LANES), 1)
    row = lax.broadcasted_iota(jnp.int32, (2 * QB, 3 * QB), 0) % QB
    column = lax.broadcasted_iota(jnp.int32, (2 * QB, 3 * QB), 1)
    near = (column >= row) & (column <= row + 2 * WINDOW)
    upper = lax.broadcasted_iota(jnp.int32, (2 * QB, 1), 0) < QB
    sinks = jnp.where(upper, first[:, HEAD : HEAD + 1], second[:, HEAD : HEAD + 1])
    half = lax.shift_left(1, group)
    start = pl.multiple_of(core * QB + 2 * QB * i, QB)
    block = first_block + core + 2 * i
    pair = q[pl.ds(start, QB), :]
    zero = jnp.zeros_like(pair)
    lower_head = jnp.where(lane < HEAD, pair, zero)
    upper_head = jnp.concatenate([pair[:, HEAD:], zero[:, HEAD:]], axis=1)
    queries = jnp.concatenate([lower_head, upper_head], axis=0)
    keys = kv_wide[pl.ds(pl.multiple_of(2 * QB * i, QB), 3 * QB), :]
    scores = lax.dot_general(
        queries, keys, (((1,), (1,)), ((), ())), preferred_element_type=jnp.float32
    )
    least = jnp.where(block == 0, QB, 0)
    limit = jnp.where(block == blocks_total - 1, 2 * QB, 3 * QB)
    valid = near & (column >= least) & (column < limit)
    scores = jnp.where(valid, scores, NEG_BIG)
    top = jnp.maximum(jnp.max(scores, axis=-1, keepdims=True), sinks)
    expo = jnp.where(valid, jnp.exp(scores - top), 0.0)
    total = jnp.sum(expo, axis=-1, keepdims=True) + jnp.exp(sinks - top)
    weights = (expo / total).astype(jnp.bfloat16)
    mixed = jnp.dot(weights, keys, preferred_element_type=jnp.float32)
    attended = jnp.concatenate([mixed[:QB, HEAD:], mixed[QB:, HEAD:]], axis=1)

    near_rows = pool_wide[pl.ds(start, QB + 2 * EDGE), :]
    size = QB + 2 * EDGE
    sums = near_rows + pltpu.roll(near_rows, 1, 0)
    chosen = sums
    for index in range(1, len(POOL_SPANS)):
        step = POOL_SPANS[index] // 4
        sums = pltpu.roll(sums, step, 0) + pltpu.roll(sums, size - step, 0)
        chosen = jnp.where(group == index, sums, chosen)
    position = block * QB + lax.broadcasted_iota(jnp.int32, (QB, 1), 0)
    counted = jnp.minimum(position + half, blocks_total * QB) - jnp.maximum(position - half, 0)
    mean = chosen[EDGE : EDGE + QB] / counted.astype(jnp.float32)
    pooled = (mean - near_rows[EDGE : EDGE + QB]) * scale
    both = jnp.concatenate([attended, pooled], axis=1).astype(jnp.bfloat16)
    for peer in range(out.shape[0]):
        out[peer] = both


def output_product(joined, own, other, out):
    core = lax.axis_index("c")
    peers = joined.shape[0]

    def product(columns):
        columns = columns.reshape(2 * peers, -1, LANES)
        total = None
        for i in range(peers):
            weights = jnp.concatenate([columns[i], columns[peers + i]], axis=1)
            part = lax.dot_general(
                joined[i], weights, (((1,), (1,)), ((), ())), preferred_element_type=jnp.float32
            )
            total = part if total is None else total + part
        return total.astype(jnp.bfloat16)

    mine, theirs = product(own[...]), product(other[...])
    out[...] = jnp.concatenate(
        [jnp.where(core == 0, mine, theirs), jnp.where(core == 0, theirs, mine)], axis=1
    )


def body(tokens, norm_gain, w_query, w_key, w_value, w_pool_in, sink_logit, pool_scale, w_out):
    rows, depth = tokens.shape
    sp_count = lax.axis_size(SP)
    bf16 = jnp.bfloat16

    key_head = lax.axis_index("x") // (lax.axis_size("x") // (w_key.shape[1] // HEAD))
    key_cols = lax.dynamic_slice_in_dim(w_key, key_head * HEAD, HEAD, 1)
    value_cols = lax.dynamic_slice_in_dim(w_value, key_head * HEAD, HEAD, 1)
    exchanged = from_everyone(jnp.concatenate([key_cols, value_cols], axis=1), SP)
    peers, pieces = exchanged.shape[:2]

    out_piece = swapped(w_out.T)

    small = jnp.concatenate([pool_scale, jnp.broadcast_to(sink_logit, (HEAD,))])[None, :]
    small = three_parts(lax.optimization_barrier(small))
    small = jnp.pad(small, ((0, EDGE - 3), (0, depth - LANES)))
    own = jnp.concatenate([w_query.T, w_pool_in.T, small], axis=0)
    other = lax.ppermute(own, "c", [(0, 1), (1, 0)])

    cosine, sine = rope_tables(lax.axis_index(SP) * rows, rows)

    at = lambda *shape: lambda *place: pl.BlockSpec(shape, lambda i: place)
    whole = lambda *shape: pl.BlockSpec(shape, lambda i: (0,) * len(shape))
    part = lambda *shape: pl.BlockSpec(shape, lambda i: (i,) + (0,) * (len(shape) - 1))
    along = lambda *shape: pl.BlockSpec(shape, lambda i: (0, i))
    shaped = lambda *shape: jax.ShapeDtypeStruct(shape, bf16)
    tables = [along(HEAD // 2, ROWS)] * 2
    normed, query, pool_in = pl.pallas_call(
        project,
        grid=(rows // ROWS,),
        in_specs=[part(ROWS, depth), whole(1, depth)] + [whole(*own.shape)] * 2 + tables,
        out_specs=[part(ROWS, depth), part(ROWS, LANES), part(ROWS, LANES)],
        out_shape=[shaped(rows, depth), shaped(rows, LANES), shaped(rows, LANES)],
        scratch_shapes=[pltpu.VMEM((2 * LANES, depth), bf16)],
        name="project",
        interpret=INTERPRET,
    )(tokens, norm_gain[None, :], own, other, cosine, sine)
    kv, send = pl.pallas_call(
        project_kv,
        grid=(rows // ROWS,),
        in_specs=[part(ROWS, depth), part(ROWS, LANES), whole(peers, pieces, LANES)] + tables,
        out_specs=[part(ROWS, LANES), whole(QB + EDGE, LANES)],
        out_shape=[shaped(rows, LANES), shaped(QB + EDGE, LANES)],
        name="project_kv",
        interpret=INTERPRET,
    )(normed, pool_in, exchanged, cosine, sine)

    pairs = [(2 * s, 2 * s + 2) for s in range(sp_count - 1)]
    pairs += [(2 * s + 3, 2 * s + 1) for s in range(sp_count - 1)]
    out_piece, send = lax.optimization_barrier((out_piece, send))
    halo = lax.ppermute(send, SP + ("c",), pairs)
    own_cols = from_everyone(out_piece, SP)

    peers_x = lax.axis_size("x")
    small_rows = at(EDGE, depth)(LANES // EDGE, 0)
    local = pl.pallas_call(
        mix,
        grid=(peers_x,),
        in_specs=[small_rows, small_rows]
        + [whole(rows, LANES)] * 3
        + [whole(QB + EDGE, LANES)],
        out_specs=pl.BlockSpec((peers_x, QB, 2 * LANES), lambda i: (0, i, 0)),
        out_shape=shaped(peers_x, rows // 2, 2 * LANES),
        scratch_shapes=[
            pltpu.VMEM((rows + QB, LANES), bf16),
            pltpu.VMEM((rows + 2 * EDGE, LANES), jnp.float32),
        ],
        name="mix",
        interpret=INTERPRET,
    )(own, other, query, kv, pool_in, halo)

    local, own_cols = lax.optimization_barrier((local, own_cols))
    other_cols = lax.ppermute(own_cols, "c", [(0, 1), (1, 0)])
    joined = lax.all_to_all(local, "x", 0, 0, tiled=True)
    pieces = out_piece.shape[0]
    width = 2 * peers // lax.axis_size("z") * pieces
    partial_cols = pl.pallas_call(
        output_product,
        grid=(1,),
        in_specs=[whole(*joined.shape)] + [whole(peers, pieces, LANES)] * 2,
        out_specs=whole(rows // 2, width),
        out_shape=shaped(rows // 2, width),
        name="output_product",
        interpret=INTERPRET,
    )(joined, own_cols, other_cols)
    return lax.all_to_all(partial_cols, "x", split_axis=0, concat_axis=1, tiled=True)


def solution(mesh):
    devices = mesh.devices
    mesh = Mesh(devices.reshape(8, devices.size // 64, 4, 2), SP + TP)
    in_specs = (
        P(SP, None),
        P(),
        P(None, TP),
        P(SP, None),
        P(SP, None),
        P(None, TP),
        P(TP),
        P(TP),
        P(TP, SP),
    )
    out_specs = P(SP + TP, None)
    return jax.shard_map(body, mesh=mesh, in_specs=in_specs, out_specs=out_specs, check_vma=False)
```

```python
import jax
import jax.numpy as jnp
from jax import lax
from jax.experimental import pallas as pl
from jax.experimental.pallas import tpu as pltpu
from jax.sharding import Mesh
from jax.sharding import PartitionSpec as P

HEAD = 64
WINDOW = 128
QB = 128
LANES = 128
ROWS = 256
EDGE = 16
POOL_SPANS = (2, 4, 8, 16)
NEG_BIG = -1e30
SP = ("z", "y")
TP = ("x", "c")
INTERPRET = False


def from_everyone(x, axis):
    peers = lax.axis_size(axis)
    return lax.all_to_all(jnp.broadcast_to(x[None], (peers, *x.shape)), axis, 0, 0, tiled=True)


def swapped(piece):
    side, depth = lax.axis_size("z"), lax.axis_size("y")
    place = lambda z, y, t: (z * depth + y) * side + t
    pairs = [
        (place(z, y, t), place(t, y, z))
        for z in range(side)
        for y in range(depth)
        for t in range(side)
    ]
    return lax.ppermute(piece, SP + TP, pairs)


def three_parts(x):
    high = lax.reduce_precision(x, 8, 7)
    middle = lax.reduce_precision(x - high, 8, 7)
    low = x - high - middle
    return jnp.concatenate([high, middle, low], axis=0).astype(jnp.bfloat16)


def rope_tables(offset, rows):
    half = HEAD // 2
    inverse = 10000.0 ** (-jnp.arange(half, dtype=jnp.float32) / half)
    positions = (offset + jnp.arange(rows)).astype(jnp.float32)
    angles = positions[None, :] * inverse[:, None]
    return jnp.cos(angles), jnp.sin(angles)


def turned(x, cosine, sine):
    lane = lax.broadcasted_iota(jnp.int32, x.shape, 1)
    wide_cosine = jnp.concatenate([cosine] * 4, axis=0).T
    wide_sine = jnp.concatenate([-sine, sine] * 2, axis=0).T
    half = HEAD // 2
    other = jnp.where(lane % HEAD < half, pltpu.roll(x, LANES - half, 1), pltpu.roll(x, half, 1))
    return x * wide_cosine + other * wide_sine


def project(tokens, gain, own, other, cosine, sine, normed_out, q_out, pool_out, weights):
    core = lax.axis_index("c")
    for place in range(2):

        @pl.when((pl.program_id(0) == 0) & (core == place))
        def _():
            for source, head in ((own, place), (other, 1 - place)):
                weights[head * HEAD : (head + 1) * HEAD] = source[:HEAD]
                weights[LANES + head * HEAD : LANES + (head + 1) * HEAD] = source[HEAD:LANES]

    values = tokens[...].astype(jnp.float32)
    center = jnp.mean(values, axis=-1, keepdims=True)
    values = values - center
    spread = jnp.mean(values * values, axis=-1, keepdims=True)
    normed = (values * lax.rsqrt(spread + 1e-06) * gain[...]).astype(jnp.bfloat16)
    normed_out[...] = normed
    sums = lax.dot_general(
        normed, weights[...], (((1,), (1,)), ((), ())), preferred_element_type=jnp.float32
    )
    query = turned(sums[:, :LANES], cosine[...], sine[...])
    q_out[...] = (query * HEAD ** (-0.5)).astype(jnp.bfloat16)
    pool_out[...] = sums[:, LANES:].astype(jnp.bfloat16)


def project_kv(normed, pool, ex, cosine, sine, kv_out, send):
    core = lax.axis_index("c")
    step = pl.program_id(0)
    rows = normed.shape[0]
    sums = jnp.dot(
        normed[...], ex[...].reshape(-1, LANES), preferred_element_type=jnp.float32
    )
    lane = lax.broadcasted_iota(jnp.int32, sums.shape, 1)
    kv = jnp.where(lane < HEAD, turned(sums, cosine[...], sine[...]), sums).astype(jnp.bfloat16)
    kv_out[...] = kv

    @pl.when((step == 0) & (core == 1))
    def _():
        send[:QB] = kv[:QB]
        send[QB:] = pool[:EDGE]

    @pl.when((step == pl.num_programs(0) - 1) & (core == 0))
    def _():
        send[:QB] = kv[rows - QB :]
        send[QB:] = pool[rows - EDGE :]


def mix(own, other, q, kv, pool, halo, out, kv_wide, pool_wide):
    core, group = lax.axis_index("c"), lax.axis_index("x")
    i = pl.program_id(0)
    rows = q.shape[0]
    blocks_total = lax.axis_size(SP) * (rows // QB)
    first_block = lax.axis_index(SP) * (rows // QB)
    mine = jnp.sum(own[:3, :LANES].astype(jnp.float32), axis=0, keepdims=True)
    theirs = jnp.sum(other[:3, :LANES].astype(jnp.float32), axis=0, keepdims=True)
    first = jnp.where(core == 0, mine, theirs)
    second = jnp.where(core == 0, theirs, mine)
    scale = jnp.concatenate([first[:, :HEAD], second[:, :HEAD]], axis=1)

    @pl.when(i == 0)
    def _():
        kv_wide[pl.ds(pl.multiple_of((1 - core) * QB, QB), rows), :] = kv[...]
        kv_wide[pl.ds(pl.multiple_of(core * rows, QB), QB), :] = halo[:QB, :]
        edge = halo[QB:, :].astype(jnp.float32)
        pool_wide[:EDGE, :] = edge
        pool_wide[EDGE : EDGE + rows, :] = pool[...].astype(jnp.float32)
        pool_wide[EDGE + rows :, :] = edge

    lane = lax.broadcasted_iota(jnp.int32, (QB, LANES), 1)
    row = lax.broadcasted_iota(jnp.int32, (2 * QB, 3 * QB), 0) % QB
    column = lax.broadcasted_iota(jnp.int32, (2 * QB, 3 * QB), 1)
    near = (column >= row) & (column <= row + 2 * WINDOW)
    upper = lax.broadcasted_iota(jnp.int32, (2 * QB, 1), 0) < QB
    sinks = jnp.where(upper, first[:, HEAD : HEAD + 1], second[:, HEAD : HEAD + 1])
    half = lax.shift_left(1, group)
    start = pl.multiple_of(core * QB + 2 * QB * i, QB)
    block = first_block + core + 2 * i
    pair = q[pl.ds(start, QB), :]
    zero = jnp.zeros_like(pair)
    lower_head = jnp.where(lane < HEAD, pair, zero)
    upper_head = jnp.concatenate([pair[:, HEAD:], zero[:, HEAD:]], axis=1)
    queries = jnp.concatenate([lower_head, upper_head], axis=0)
    keys = kv_wide[pl.ds(pl.multiple_of(2 * QB * i, QB), 3 * QB), :]
    scores = lax.dot_general(
        queries, keys, (((1,), (1,)), ((), ())), preferred_element_type=jnp.float32
    )
    least = jnp.where(block == 0, QB, 0)
    limit = jnp.where(block == blocks_total - 1, 2 * QB, 3 * QB)
    valid = near & (column >= least) & (column < limit)
    scores = jnp.where(valid, scores, NEG_BIG)
    top = jnp.maximum(jnp.max(scores, axis=-1, keepdims=True), sinks)
    expo = jnp.where(valid, jnp.exp(scores - top), 0.0)
    total = jnp.sum(expo, axis=-1, keepdims=True) + jnp.exp(sinks - top)
    weights = (expo / total).astype(jnp.bfloat16)
    mixed = jnp.dot(weights, keys, preferred_element_type=jnp.float32)
    attended = jnp.concatenate([mixed[:QB, HEAD:], mixed[QB:, HEAD:]], axis=1)

    near_rows = pool_wide[pl.ds(start, QB + 2 * EDGE), :]
    size = QB + 2 * EDGE
    sums = near_rows + pltpu.roll(near_rows, 1, 0)
    chosen = sums
    for index in range(1, len(POOL_SPANS)):
        step = POOL_SPANS[index] // 4
        sums = pltpu.roll(sums, step, 0) + pltpu.roll(sums, size - step, 0)
        chosen = jnp.where(group == index, sums, chosen)
    position = block * QB + lax.broadcasted_iota(jnp.int32, (QB, 1), 0)
    counted = jnp.minimum(position + half, blocks_total * QB) - jnp.maximum(position - half, 0)
    mean = chosen[EDGE : EDGE + QB] / counted.astype(jnp.float32)
    pooled = (mean - near_rows[EDGE : EDGE + QB]) * scale
    both = jnp.concatenate([attended, pooled], axis=1).astype(jnp.bfloat16)
    for peer in range(out.shape[0]):
        out[peer] = both


def output_product(joined, own, other, out):
    core = lax.axis_index("c")
    peers = joined.shape[0]

    def product(columns):
        columns = columns.reshape(2 * peers, -1, LANES)
        total = None
        for i in range(peers):
            weights = jnp.concatenate([columns[i], columns[peers + i]], axis=1)
            part = lax.dot_general(
                joined[i], weights, (((1,), (1,)), ((), ())), preferred_element_type=jnp.float32
            )
            total = part if total is None else total + part
        return total.astype(jnp.bfloat16)

    mine, theirs = product(own[...]), product(other[...])
    out[...] = jnp.concatenate(
        [jnp.where(core == 0, mine, theirs), jnp.where(core == 0, theirs, mine)], axis=1
    )


def body(tokens, norm_gain, w_query, w_key, w_value, w_pool_in, sink_logit, pool_scale, w_out):
    rows, depth = tokens.shape
    sp_count = lax.axis_size(SP)
    bf16 = jnp.bfloat16

    key_head = lax.axis_index("x") // (lax.axis_size("x") // (w_key.shape[1] // HEAD))
    key_cols = lax.dynamic_slice_in_dim(w_key, key_head * HEAD, HEAD, 1)
    value_cols = lax.dynamic_slice_in_dim(w_value, key_head * HEAD, HEAD, 1)
    exchanged = from_everyone(jnp.concatenate([key_cols, value_cols], axis=1), SP)
    peers, pieces = exchanged.shape[:2]

    out_piece = swapped(w_out.T)

    small = jnp.concatenate([pool_scale, jnp.broadcast_to(sink_logit, (HEAD,))])[None, :]
    small = three_parts(lax.optimization_barrier(small))
    small = jnp.pad(small, ((0, EDGE - 3), (0, depth - LANES)))
    own = jnp.concatenate([w_query.T, w_pool_in.T, small], axis=0)
    other = lax.ppermute(own, "c", [(0, 1), (1, 0)])

    cosine, sine = rope_tables(lax.axis_index(SP) * rows, rows)

    exchanged, out_piece, cosine, sine, other = lax.optimization_barrier(
        (exchanged, out_piece, cosine, sine, other)
    )
    own_cols = from_everyone(out_piece, SP)

    at = lambda *shape: lambda *place: pl.BlockSpec(shape, lambda i: place)
    whole = lambda *shape: pl.BlockSpec(shape, lambda i: (0,) * len(shape))
    part = lambda *shape: pl.BlockSpec(shape, lambda i: (i,) + (0,) * (len(shape) - 1))
    along = lambda *shape: pl.BlockSpec(shape, lambda i: (0, i))
    shaped = lambda *shape: jax.ShapeDtypeStruct(shape, bf16)
    tables = [along(HEAD // 2, ROWS)] * 2
    normed, query, pool_in = pl.pallas_call(
        project,
        grid=(rows // ROWS,),
        in_specs=[part(ROWS, depth), whole(1, depth)] + [whole(*own.shape)] * 2 + tables,
        out_specs=[part(ROWS, depth), part(ROWS, LANES), part(ROWS, LANES)],
        out_shape=[shaped(rows, depth), shaped(rows, LANES), shaped(rows, LANES)],
        scratch_shapes=[pltpu.VMEM((2 * LANES, depth), bf16)],
        name="project",
        interpret=INTERPRET,
    )(tokens, norm_gain[None, :], own, other, cosine, sine)
    kv, send = pl.pallas_call(
        project_kv,
        grid=(rows // ROWS,),
        in_specs=[part(ROWS, depth), part(ROWS, LANES), whole(peers, pieces, LANES)] + tables,
        out_specs=[part(ROWS, LANES), whole(QB + EDGE, LANES)],
        out_shape=[shaped(rows, LANES), shaped(QB + EDGE, LANES)],
        name="project_kv",
        interpret=INTERPRET,
    )(normed, pool_in, exchanged, cosine, sine)

    pairs = [(2 * s, 2 * s + 2) for s in range(sp_count - 1)]
    pairs += [(2 * s + 3, 2 * s + 1) for s in range(sp_count - 1)]
    halo = lax.ppermute(send, SP + ("c",), pairs)
    other_cols = lax.ppermute(own_cols, "c", [(0, 1), (1, 0)])

    peers_x = lax.axis_size("x")
    small_rows = at(EDGE, depth)(LANES // EDGE, 0)
    local = pl.pallas_call(
        mix,
        grid=(peers_x,),
        in_specs=[small_rows, small_rows]
        + [whole(rows, LANES)] * 3
        + [whole(QB + EDGE, LANES)],
        out_specs=pl.BlockSpec((peers_x, QB, 2 * LANES), lambda i: (0, i, 0)),
        out_shape=shaped(peers_x, rows // 2, 2 * LANES),
        scratch_shapes=[
            pltpu.VMEM((rows + QB, LANES), bf16),
            pltpu.VMEM((rows + 2 * EDGE, LANES), jnp.float32),
        ],
        name="mix",
        interpret=INTERPRET,
    )(own, other, query, kv, pool_in, halo)

    local, other_cols = lax.optimization_barrier((local, other_cols))
    joined = lax.all_to_all(local, "x", 0, 0, tiled=True)
    pieces = out_piece.shape[0]
    width = 2 * peers // lax.axis_size("z") * pieces
    partial_cols = pl.pallas_call(
        output_product,
        grid=(1,),
        in_specs=[whole(*joined.shape)] + [whole(peers, pieces, LANES)] * 2,
        out_specs=whole(rows // 2, width),
        out_shape=shaped(rows // 2, width),
        name="output_product",
        interpret=INTERPRET,
    )(joined, own_cols, other_cols)
    return lax.all_to_all(partial_cols, "x", split_axis=0, concat_axis=1, tiled=True)


def solution(mesh):
    devices = mesh.devices
    mesh = Mesh(devices.reshape(8, devices.size // 64, 4, 2), SP + TP)
    in_specs = (
        P(SP, None),
        P(),
        P(None, TP),
        P(SP, None),
        P(SP, None),
        P(None, TP),
        P(TP),
        P(TP),
        P(TP, SP),
    )
    out_specs = P(SP + TP, None)
    return jax.shard_map(body, mesh=mesh, in_specs=in_specs, out_specs=out_specs, check_vma=False)
```

```python
import jax
import jax.numpy as jnp
from jax import lax
from jax.experimental import pallas as pl
from jax.experimental.pallas import tpu as pltpu
from jax.sharding import Mesh
from jax.sharding import PartitionSpec as P

HEAD = 64
WINDOW = 128
QB = 128
LANES = 128
ROWS = 256
STEP = 2
EDGE = 16
POOL_SPANS = (2, 4, 8, 16)
NEG_BIG = -1e30
SP = ("z", "y")
TP = ("x", "c")
INTERPRET = False


def from_everyone(x, axis):
    peers = lax.axis_size(axis)
    return lax.all_to_all(jnp.broadcast_to(x[None], (peers, *x.shape)), axis, 0, 0, tiled=True)


def swapped(piece):
    side, depth = lax.axis_size("z"), lax.axis_size("y")
    place = lambda z, y, t: (z * depth + y) * side + t
    pairs = [
        (place(z, y, t), place(t, y, z))
        for z in range(side)
        for y in range(depth)
        for t in range(side)
    ]
    return lax.ppermute(piece, SP + TP, pairs)


def three_parts(x):
    high = lax.reduce_precision(x, 8, 7)
    middle = lax.reduce_precision(x - high, 8, 7)
    low = x - high - middle
    return jnp.concatenate([high, middle, low], axis=0).astype(jnp.bfloat16)


def rope_tables(offset, rows):
    half = HEAD // 2
    inverse = 10000.0 ** (-jnp.arange(half, dtype=jnp.float32) / half)
    positions = (offset + jnp.arange(rows)).astype(jnp.float32)
    angles = positions[None, :] * inverse[:, None]
    return jnp.cos(angles), jnp.sin(angles)


def turned(x, cosine, sine):
    lane = lax.broadcasted_iota(jnp.int32, x.shape, 1)
    wide_cosine = jnp.concatenate([cosine] * 4, axis=0).T
    wide_sine = jnp.concatenate([-sine, sine] * 2, axis=0).T
    half = HEAD // 2
    other = jnp.where(lane % HEAD < half, pltpu.roll(x, LANES - half, 1), pltpu.roll(x, half, 1))
    return x * wide_cosine + other * wide_sine


def project(tokens, gain, own, other, cosine, sine, normed_out, q_out, pool_out, weights):
    core = lax.axis_index("c")
    for place in range(2):

        @pl.when((pl.program_id(0) == 0) & (core == place))
        def _():
            for source, head in ((own, place), (other, 1 - place)):
                weights[head * HEAD : (head + 1) * HEAD] = source[:HEAD]
                weights[LANES + head * HEAD : LANES + (head + 1) * HEAD] = source[HEAD:LANES]

    values = tokens[...].astype(jnp.float32)
    center = jnp.mean(values, axis=-1, keepdims=True)
    values = values - center
    spread = jnp.mean(values * values, axis=-1, keepdims=True)
    normed = (values * lax.rsqrt(spread + 1e-06) * gain[...]).astype(jnp.bfloat16)
    normed_out[...] = normed
    sums = lax.dot_general(
        normed, weights[...], (((1,), (1,)), ((), ())), preferred_element_type=jnp.float32
    )
    query = turned(sums[:, :LANES], cosine[...], sine[...])
    q_out[...] = (query * HEAD ** (-0.5)).astype(jnp.bfloat16)
    pool_out[...] = sums[:, LANES:].astype(jnp.bfloat16)


def project_kv(normed, pool, ex, cosine, sine, kv_out, send):
    core = lax.axis_index("c")
    step = pl.program_id(0)
    rows = normed.shape[0]
    sums = jnp.dot(
        normed[...], ex[...].reshape(-1, LANES), preferred_element_type=jnp.float32
    )
    lane = lax.broadcasted_iota(jnp.int32, sums.shape, 1)
    kv = jnp.where(lane < HEAD, turned(sums, cosine[...], sine[...]), sums).astype(jnp.bfloat16)
    kv_out[...] = kv

    @pl.when((step == 0) & (core == 1))
    def _():
        send[:QB] = kv[:QB]
        send[QB:] = pool[:EDGE]

    @pl.when((step == pl.num_programs(0) - 1) & (core == 0))
    def _():
        send[:QB] = kv[rows - QB :]
        send[QB:] = pool[rows - EDGE :]


def mix(own, other, q, kv, pool, halo, out, kv_wide, pool_wide):
    core, group = lax.axis_index("c"), lax.axis_index("x")
    rows = q.shape[0]
    blocks_total = lax.axis_size(SP) * (rows // QB)
    first_block = lax.axis_index(SP) * (rows // QB)
    mine = jnp.sum(own[:3, :LANES].astype(jnp.float32), axis=0, keepdims=True)
    theirs = jnp.sum(other[:3, :LANES].astype(jnp.float32), axis=0, keepdims=True)
    first = jnp.where(core == 0, mine, theirs)
    second = jnp.where(core == 0, theirs, mine)
    scale = jnp.concatenate([first[:, :HEAD], second[:, :HEAD]], axis=1)

    @pl.when(pl.program_id(0) == 0)
    def _():
        kv_wide[pl.ds(pl.multiple_of((1 - core) * QB, QB), rows), :] = kv[...]
        kv_wide[pl.ds(pl.multiple_of(core * rows, QB), QB), :] = halo[:QB, :]
        edge = halo[QB:, :].astype(jnp.float32)
        pool_wide[:EDGE, :] = edge
        pool_wide[EDGE : EDGE + rows, :] = pool[...].astype(jnp.float32)
        pool_wide[EDGE + rows :, :] = edge

    lane = lax.broadcasted_iota(jnp.int32, (QB, LANES), 1)
    row = lax.broadcasted_iota(jnp.int32, (2 * QB, 3 * QB), 0) % QB
    column = lax.broadcasted_iota(jnp.int32, (2 * QB, 3 * QB), 1)
    near = (column >= row) & (column <= row + 2 * WINDOW)
    upper = lax.broadcasted_iota(jnp.int32, (2 * QB, 1), 0) < QB
    sinks = jnp.where(upper, first[:, HEAD : HEAD + 1], second[:, HEAD : HEAD + 1])
    half = lax.shift_left(1, group)
    for j in range(STEP):
        i = pl.program_id(0) * STEP + j
        start = pl.multiple_of(core * QB + 2 * QB * i, QB)
        block = first_block + core + 2 * i
        pair = q[pl.ds(start, QB), :]
        zero = jnp.zeros_like(pair)
        lower_head = jnp.where(lane < HEAD, pair, zero)
        upper_head = jnp.concatenate([pair[:, HEAD:], zero[:, HEAD:]], axis=1)
        queries = jnp.concatenate([lower_head, upper_head], axis=0)
        keys = kv_wide[pl.ds(pl.multiple_of(2 * QB * i, QB), 3 * QB), :]
        scores = lax.dot_general(
            queries, keys, (((1,), (1,)), ((), ())), preferred_element_type=jnp.float32
        )
        least = jnp.where(block == 0, QB, 0)
        limit = jnp.where(block == blocks_total - 1, 2 * QB, 3 * QB)
        valid = near & (column >= least) & (column < limit)
        scores = jnp.where(valid, scores, NEG_BIG)
        top = jnp.maximum(jnp.max(scores, axis=-1, keepdims=True), sinks)
        expo = jnp.where(valid, jnp.exp(scores - top), 0.0)
        total = jnp.sum(expo, axis=-1, keepdims=True) + jnp.exp(sinks - top)
        weights = (expo / total).astype(jnp.bfloat16)
        mixed = jnp.dot(weights, keys, preferred_element_type=jnp.float32)
        attended = jnp.concatenate([mixed[:QB, HEAD:], mixed[QB:, HEAD:]], axis=1)

        near_rows = pool_wide[pl.ds(start, QB + 2 * EDGE), :]
        size = QB + 2 * EDGE
        sums = near_rows + pltpu.roll(near_rows, 1, 0)
        chosen = sums
        for index in range(1, len(POOL_SPANS)):
            step = POOL_SPANS[index] // 4
            sums = pltpu.roll(sums, step, 0) + pltpu.roll(sums, size - step, 0)
            chosen = jnp.where(group == index, sums, chosen)
        position = block * QB + lax.broadcasted_iota(jnp.int32, (QB, 1), 0)
        counted = jnp.minimum(position + half, blocks_total * QB) - jnp.maximum(position - half, 0)
        mean = chosen[EDGE : EDGE + QB] / counted.astype(jnp.float32)
        pooled = (mean - near_rows[EDGE : EDGE + QB]) * scale
        both = jnp.concatenate([attended, pooled], axis=1).astype(jnp.bfloat16)
        for peer in range(out.shape[0]):
            out[peer, j * QB : (j + 1) * QB] = both


def body(tokens, norm_gain, w_query, w_key, w_value, w_pool_in, sink_logit, pool_scale, w_out):
    rows, depth = tokens.shape
    sp_count = lax.axis_size(SP)
    bf16 = jnp.bfloat16

    key_head = lax.axis_index("x") // (lax.axis_size("x") // (w_key.shape[1] // HEAD))
    key_cols = lax.dynamic_slice_in_dim(w_key, key_head * HEAD, HEAD, 1)
    value_cols = lax.dynamic_slice_in_dim(w_value, key_head * HEAD, HEAD, 1)
    exchanged = from_everyone(jnp.concatenate([key_cols, value_cols], axis=1), SP)
    peers, pieces = exchanged.shape[:2]

    out_piece = swapped(w_out.T)

    small = jnp.concatenate([pool_scale, jnp.broadcast_to(sink_logit, (HEAD,))])[None, :]
    small = three_parts(lax.optimization_barrier(small))
    small = jnp.pad(small, ((0, EDGE - 3), (0, depth - LANES)))
    own = jnp.concatenate([w_query.T, w_pool_in.T, small], axis=0)
    other = lax.ppermute(own, "c", [(0, 1), (1, 0)])

    cosine, sine = rope_tables(lax.axis_index(SP) * rows, rows)

    at = lambda *shape: lambda *place: pl.BlockSpec(shape, lambda i: place)
    whole = lambda *shape: pl.BlockSpec(shape, lambda i: (0,) * len(shape))
    part = lambda *shape: pl.BlockSpec(shape, lambda i: (i,) + (0,) * (len(shape) - 1))
    along = lambda *shape: pl.BlockSpec(shape, lambda i: (0, i))
    shaped = lambda *shape: jax.ShapeDtypeStruct(shape, bf16)
    tables = [along(HEAD // 2, ROWS)] * 2
    normed, query, pool_in = pl.pallas_call(
        project,
        grid=(rows // ROWS,),
        in_specs=[part(ROWS, depth), whole(1, depth)] + [whole(*own.shape)] * 2 + tables,
        out_specs=[part(ROWS, depth), part(ROWS, LANES), part(ROWS, LANES)],
        out_shape=[shaped(rows, depth), shaped(rows, LANES), shaped(rows, LANES)],
        scratch_shapes=[pltpu.VMEM((2 * LANES, depth), bf16)],
        name="project",
        interpret=INTERPRET,
    )(tokens, norm_gain[None, :], own, other, cosine, sine)
    exchanged, out_piece, normed = lax.optimization_barrier((exchanged, out_piece, normed))
    own_cols = from_everyone(out_piece, SP)
    kv, send = pl.pallas_call(
        project_kv,
        grid=(rows // ROWS,),
        in_specs=[part(ROWS, depth), part(ROWS, LANES), whole(peers, pieces, LANES)] + tables,
        out_specs=[part(ROWS, LANES), whole(QB + EDGE, LANES)],
        out_shape=[shaped(rows, LANES), shaped(QB + EDGE, LANES)],
        name="project_kv",
        interpret=INTERPRET,
    )(normed, pool_in, exchanged, cosine, sine)

    pairs = [(2 * s, 2 * s + 2) for s in range(sp_count - 1)]
    pairs += [(2 * s + 3, 2 * s + 1) for s in range(sp_count - 1)]
    halo = lax.ppermute(send, SP + ("c",), pairs)
    peers_x = lax.axis_size("x")
    small_rows = at(EDGE, depth)(LANES // EDGE, 0)
    local = pl.pallas_call(
        mix,
        grid=(rows // (2 * QB * STEP),),
        in_specs=[small_rows, small_rows]
        + [whole(rows, LANES)] * 3
        + [whole(QB + EDGE, LANES)],
        out_specs=pl.BlockSpec((peers_x, STEP * QB, 2 * LANES), lambda i: (0, i, 0)),
        out_shape=shaped(peers_x, rows // 2, 2 * LANES),
        scratch_shapes=[
            pltpu.VMEM((rows + QB, LANES), bf16),
            pltpu.VMEM((rows + 2 * EDGE, LANES), jnp.float32),
        ],
        name="mix",
        interpret=INTERPRET,
    )(own, other, query, kv, pool_in, halo)

    local, own_cols = lax.optimization_barrier((local, own_cols))
    other_cols = lax.ppermute(own_cols, "c", [(0, 1), (1, 0)])
    joined = lax.all_to_all(local, "x", 0, 0, tiled=True)

    def matched(columns):
        columns = columns.reshape(2, peers_x, -1, LANES)
        return jnp.concatenate([columns[0], columns[1]], axis=2)

    core = lax.axis_index("c")
    mine, theirs = matched(own_cols), matched(other_cols)
    columns = jnp.concatenate(
        [jnp.where(core == 0, mine, theirs), jnp.where(core == 0, theirs, mine)], axis=1
    )
    partial_cols = jnp.einsum(
        "ptc,pnc->tn", joined, columns, preferred_element_type=jnp.float32
    ).astype(bf16)
    return lax.all_to_all(partial_cols, "x", split_axis=0, concat_axis=1, tiled=True)


def solution(mesh):
    devices = mesh.devices
    mesh = Mesh(devices.reshape(8, devices.size // 64, 4, 2), SP + TP)
    in_specs = (
        P(SP, None),
        P(),
        P(None, TP),
        P(SP, None),
        P(SP, None),
        P(None, TP),
        P(TP),
        P(TP),
        P(TP, SP),
    )
    out_specs = P(SP + TP, None)
    return jax.shard_map(body, mesh=mesh, in_specs=in_specs, out_specs=out_specs, check_vma=False)
```

```python
import functools

import jax
import jax.numpy as jnp
import numpy as np
from jax import lax
from jax.experimental import pallas as pl
from jax.experimental.pallas import tpu as pltpu
from jax.sharding import Mesh
from jax.sharding import PartitionSpec as P

HEAD = 64
WINDOW = 128
QB = 128
LANES = 128
ROWS = 256
STEPS = 4
EDGE = 16
POOL_SPANS = (2, 4, 8, 16)
NEG_BIG = -1e30
SP = ("z", "y")
TP = ("x", "c")
INTERPRET = False


def from_everyone(x, axis):
    peers = lax.axis_size(axis)
    return lax.all_to_all(jnp.broadcast_to(x[None], (peers, *x.shape)), axis, 0, 0, tiled=True)


def swapped(piece):
    side, depth = lax.axis_size("z"), lax.axis_size("y")
    place = lambda z, y, t: (z * depth + y) * side + t
    pairs = [
        (place(z, y, t), place(t, y, z))
        for z in range(side)
        for y in range(depth)
        for t in range(side)
    ]
    return lax.ppermute(piece, SP + TP, pairs)


def three_parts(x):
    high = lax.reduce_precision(x, 8, 7)
    middle = lax.reduce_precision(x - high, 8, 7)
    low = x - high - middle
    return jnp.concatenate([high, middle, low], axis=0).astype(jnp.bfloat16)


def rope_tables(offset, rows):
    half = HEAD // 2
    inverse = 10000.0 ** (-jnp.arange(half, dtype=jnp.float32) / half)
    starts = (offset + QB * jnp.arange(rows // QB)).astype(jnp.float32)
    coarse = starts[None, :] * inverse[:, None]
    exact = 10000.0 ** (-np.arange(half) / half)
    fine = np.arange(QB)[None, :] * exact[:, None]
    fine = jnp.asarray(np.stack([np.cos(fine), np.sin(fine)]), jnp.float32)
    return jnp.stack([jnp.cos(coarse), jnp.sin(coarse)]), fine


def turned(x, coarse, fine, first_block):
    places = lax.broadcasted_iota(jnp.int32, coarse.shape[1:], 1)
    cosines, sines = [], []
    for block in range(x.shape[0] // QB):
        here = places == first_block + block
        cosine = jnp.sum(jnp.where(here, coarse[0], 0.0), axis=1, keepdims=True)
        sine = jnp.sum(jnp.where(here, coarse[1], 0.0), axis=1, keepdims=True)
        cosines.append(cosine * fine[0] - sine * fine[1])
        sines.append(sine * fine[0] + cosine * fine[1])
    cosine, sine = jnp.concatenate(cosines, axis=1), jnp.concatenate(sines, axis=1)
    lane = lax.broadcasted_iota(jnp.int32, x.shape, 1)
    wide_cosine = jnp.concatenate([cosine] * 4, axis=0).T
    wide_sine = jnp.concatenate([-sine, sine] * 2, axis=0).T
    half = HEAD // 2
    other = jnp.where(lane % HEAD < half, pltpu.roll(x, LANES - half, 1), pltpu.roll(x, half, 1))
    return x * wide_cosine + other * wide_sine


def project(tokens, gain, own, other, coarse, fine, normed_out, q_out, pool_out, weights):
    core = lax.axis_index("c")
    for place in range(2):

        @pl.when((pl.program_id(0) == 0) & (core == place))
        def _():
            for source, head in ((own, place), (other, 1 - place)):
                weights[head * HEAD : (head + 1) * HEAD] = source[:HEAD]
                weights[LANES + head * HEAD : LANES + (head + 1) * HEAD] = source[HEAD:LANES]

    values = tokens[...].astype(jnp.float32)
    center = jnp.mean(values, axis=-1, keepdims=True)
    values = values - center
    spread = jnp.mean(values * values, axis=-1, keepdims=True)
    normed = (values * lax.rsqrt(spread + 1e-06) * gain[...]).astype(jnp.bfloat16)
    normed_out[...] = normed
    sums = lax.dot_general(
        normed, weights[...], (((1,), (1,)), ((), ())), preferred_element_type=jnp.float32
    )
    first_block = pl.program_id(0) * (ROWS // QB)
    query = turned(sums[:, :LANES], coarse[...], fine[...], first_block)
    q_out[...] = (query * HEAD ** (-0.5)).astype(jnp.bfloat16)
    pool_out[...] = sums[:, LANES:].astype(jnp.bfloat16)


def project_kv(normed, pool, ex, coarse, fine, kv_out, send, total):
    step, rows = pl.program_id(0), normed.shape[0]
    part = jnp.dot(normed[...], ex[...].reshape(-1, LANES), preferred_element_type=jnp.float32)

    @pl.when(step == 0)
    def _():
        total[...] = part

    @pl.when(step > 0)
    def _():
        total[...] += part

    @pl.when(step == pl.num_programs(0) - 1)
    def _():
        core, sums = lax.axis_index("c"), total[...]
        lane = lax.broadcasted_iota(jnp.int32, sums.shape, 1)
        kv = jnp.where(lane < HEAD, turned(sums, coarse[...], fine[...], 0), sums)
        kv = kv.astype(jnp.bfloat16)
        kv_out[...] = kv
        send[:QB] = jnp.where(core == 0, kv[rows - QB :], kv[:QB])
        send[QB:] = jnp.where(core == 0, pool[rows - EDGE :], pool[:EDGE])


def mix(inner, own, other, q, kv, pool, *rest):
    out, kv_wide, pool_wide, both, sems = rest[-5:]
    core, group = lax.axis_index("c"), lax.axis_index("x")
    rows = q.shape[0]
    blocks_total = lax.axis_size(SP) * (rows // QB)
    first_block = lax.axis_index(SP) * (rows // QB)
    mine = jnp.sum(own[:3, :LANES].astype(jnp.float32), axis=0, keepdims=True)
    theirs = jnp.sum(other[:3, :LANES].astype(jnp.float32), axis=0, keepdims=True)
    first = jnp.where(core == 0, mine, theirs)
    second = jnp.where(core == 0, theirs, mine)
    scale = jnp.concatenate([first[:, :HEAD], second[:, :HEAD]], axis=1)
    kv_wide[pl.ds(pl.multiple_of((1 - core) * QB, QB), rows), :] = kv[...]
    pool_wide[EDGE : EDGE + rows, :] = pool[...].astype(jnp.float32)
    if not inner:
        halo = rest[0]
        kv_wide[pl.ds(pl.multiple_of(core * rows, QB), QB), :] = halo[:QB, :]
        edge = halo[QB:, :].astype(jnp.float32)
        pool_wide[:EDGE, :] = edge
        pool_wide[EDGE + rows :, :] = edge
    lane = lax.broadcasted_iota(jnp.int32, (QB, LANES), 1)
    row = lax.broadcasted_iota(jnp.int32, (2 * QB, 3 * QB), 0) % QB
    column = lax.broadcasted_iota(jnp.int32, (2 * QB, 3 * QB), 1)
    near = (column >= row) & (column <= row + 2 * WINDOW)
    upper = lax.broadcasted_iota(jnp.int32, (2 * QB, 1), 0) < QB
    sinks = jnp.where(upper, first[:, HEAD : HEAD + 1], second[:, HEAD : HEAD + 1])
    half = lax.shift_left(1, group)
    copies = []
    for j in range(both.shape[0]):
        i = 1 - core + j if inner else core * (rows // (2 * QB) - 1)
        start = pl.multiple_of(core * QB + 2 * QB * i, QB)
        block = first_block + core + 2 * i
        pair = q[pl.ds(start, QB), :]
        zero = jnp.zeros_like(pair)
        lower_head = jnp.where(lane < HEAD, pair, zero)
        upper_head = jnp.concatenate([pair[:, HEAD:], zero[:, HEAD:]], axis=1)
        queries = jnp.concatenate([lower_head, upper_head], axis=0)
        keys = kv_wide[pl.ds(pl.multiple_of(2 * QB * i, QB), 3 * QB), :]
        scores = lax.dot_general(
            queries, keys, (((1,), (1,)), ((), ())), preferred_element_type=jnp.float32
        )
        least = jnp.where(block == 0, QB, 0)
        limit = jnp.where(block == blocks_total - 1, 2 * QB, 3 * QB)
        valid = near & (column >= least) & (column < limit)
        scores = jnp.where(valid, scores, NEG_BIG)
        top = jnp.maximum(jnp.max(scores, axis=-1, keepdims=True), sinks)
        expo = jnp.where(valid, jnp.exp(scores - top), 0.0)
        total = jnp.sum(expo, axis=-1, keepdims=True) + jnp.exp(sinks - top)
        weights = (expo / total).astype(jnp.bfloat16)
        mixed = jnp.dot(weights, keys, preferred_element_type=jnp.float32)
        attended = jnp.concatenate([mixed[:QB, HEAD:], mixed[QB:, HEAD:]], axis=1)

        near_rows = pool_wide[pl.ds(start, QB + 2 * EDGE), :]
        size = QB + 2 * EDGE
        sums = near_rows + pltpu.roll(near_rows, 1, 0)
        chosen = sums
        for index in range(1, len(POOL_SPANS)):
            step = POOL_SPANS[index] // 4
            sums = pltpu.roll(sums, step, 0) + pltpu.roll(sums, size - step, 0)
            chosen = jnp.where(group == index, sums, chosen)
        position = block * QB + lax.broadcasted_iota(jnp.int32, (QB, 1), 0)
        counted = jnp.minimum(position + half, blocks_total * QB) - jnp.maximum(position - half, 0)
        mean = chosen[EDGE : EDGE + QB] / counted.astype(jnp.float32)
        pooled = (mean - near_rows[EDGE : EDGE + QB]) * scale
        both[j] = jnp.concatenate([attended, pooled], axis=1).astype(jnp.bfloat16)
        for peer in range(out.shape[0]):
            target = out.at[peer, pl.ds(pl.multiple_of(i * QB, QB), QB)]
            copies.append(pltpu.make_async_copy(both.at[j], target, sems.at[j, peer]))
            copies[-1].start()
    for copy in copies:
        copy.wait()


def body(tokens, norm_gain, w_query, w_key, w_value, w_pool_in, sink_logit, pool_scale, w_out):
    rows, depth = tokens.shape
    sp_count = lax.axis_size(SP)
    bf16 = jnp.bfloat16

    key_head = lax.axis_index("x") // (lax.axis_size("x") // (w_key.shape[1] // HEAD))
    key_cols = lax.dynamic_slice_in_dim(w_key, key_head * HEAD, HEAD, 1)
    value_cols = lax.dynamic_slice_in_dim(w_value, key_head * HEAD, HEAD, 1)
    exchanged = from_everyone(jnp.concatenate([key_cols, value_cols], axis=1), SP)
    peers, pieces = exchanged.shape[:2]

    out_piece = swapped(w_out.T)

    small = jnp.concatenate([pool_scale, jnp.broadcast_to(sink_logit, (HEAD,))])[None, :]
    small = three_parts(lax.optimization_barrier(small))
    small = jnp.pad(small, ((0, EDGE - 3), (0, depth - LANES)))
    own = jnp.concatenate([w_query.T, w_pool_in.T, small], axis=0)
    other = lax.ppermute(own, "c", [(0, 1), (1, 0)])

    coarse, fine = rope_tables(lax.axis_index(SP) * rows, rows)

    at = lambda *shape: lambda *place: pl.BlockSpec(shape, lambda i: place)
    whole = lambda *shape: pl.BlockSpec(shape, lambda i: (0,) * len(shape))
    part = lambda *shape: pl.BlockSpec(shape, lambda i: (i,) + (0,) * (len(shape) - 1))
    along = lambda *shape: pl.BlockSpec(shape, lambda i: (0, i))
    shaped = lambda *shape: jax.ShapeDtypeStruct(shape, bf16)
    tables = [whole(*coarse.shape), whole(*fine.shape)]
    normed, query, pool_in = pl.pallas_call(
        project,
        grid=(rows // ROWS,),
        in_specs=[part(ROWS, depth), whole(1, depth)] + [whole(*own.shape)] * 2 + tables,
        out_specs=[part(ROWS, depth), part(ROWS, LANES), part(ROWS, LANES)],
        out_shape=[shaped(rows, depth), shaped(rows, LANES), shaped(rows, LANES)],
        scratch_shapes=[pltpu.VMEM((2 * LANES, depth), bf16)],
        name="project",
        interpret=INTERPRET,
    )(tokens, norm_gain[None, :], own, other, coarse, fine)
    exchanged, out_piece, normed = lax.optimization_barrier((exchanged, out_piece, normed))
    own_cols = from_everyone(out_piece, SP)
    kv, send = pl.pallas_call(
        project_kv,
        grid=(STEPS,),
        in_specs=[along(rows, depth // STEPS), whole(rows, LANES)]
        + [part(peers // STEPS, pieces, LANES)]
        + tables,
        out_specs=[whole(rows, LANES), whole(QB + EDGE, LANES)],
        out_shape=[shaped(rows, LANES), shaped(QB + EDGE, LANES)],
        scratch_shapes=[pltpu.VMEM((rows, LANES), jnp.float32)],
        name="project_kv",
        interpret=INTERPRET,
    )(normed, pool_in, exchanged, coarse, fine)

    pairs = [(2 * s, 2 * s + 2) for s in range(sp_count - 1)]
    pairs += [(2 * s + 3, 2 * s + 1) for s in range(sp_count - 1)]
    halo = lax.ppermute(send, SP + ("c",), pairs)
    peers_x = lax.axis_size("x")
    small_rows = at(EDGE, depth)(LANES // EDGE, 0)
    anywhere = pl.BlockSpec(memory_space=pl.ANY)
    local_specs = [small_rows, small_rows] + [whole(rows, LANES)] * 3

    def mixed(inner, *more):
        blocks = rows // (2 * QB) - 1 if inner else 1
        return pl.pallas_call(
            functools.partial(mix, inner),
            grid=(1,),
            in_specs=local_specs + ([] if inner else [whole(QB + EDGE, LANES), anywhere]),
            out_specs=anywhere,
            out_shape=shaped(peers_x, rows // 2, 2 * LANES),
            input_output_aliases={} if inner else {6: 0},
            scratch_shapes=[
                pltpu.VMEM((rows + QB, LANES), bf16),
                pltpu.VMEM((rows + 2 * EDGE, LANES), jnp.float32),
                pltpu.VMEM((blocks, QB, 2 * LANES), bf16),
                pltpu.SemaphoreType.DMA((blocks, peers_x)),
            ],
            name="mix_inner" if inner else "mix_outer",
            interpret=INTERPRET,
        )(own, other, query, kv, pool_in, *more)

    local = mixed(True)
    local = mixed(False, halo, local)

    local, own_cols = lax.optimization_barrier((local, own_cols))
    other_cols = lax.ppermute(own_cols, "c", [(0, 1), (1, 0)])
    joined = lax.all_to_all(local, "x", 0, 0, tiled=True)

    def matched(columns):
        columns = columns.reshape(2, peers_x, -1, LANES)
        return jnp.concatenate([columns[0], columns[1]], axis=2)

    core = lax.axis_index("c")
    mine, theirs = matched(own_cols), matched(other_cols)
    columns = jnp.concatenate(
        [jnp.where(core == 0, mine, theirs), jnp.where(core == 0, theirs, mine)], axis=1
    )
    partial_cols = jnp.einsum(
        "ptc,pnc->tn", joined, columns, preferred_element_type=jnp.float32
    ).astype(bf16)
    return lax.all_to_all(partial_cols, "x", split_axis=0, concat_axis=1, tiled=True)


def solution(mesh):
    devices = mesh.devices
    mesh = Mesh(devices.reshape(8, devices.size // 64, 4, 2), SP + TP)
    in_specs = (
        P(SP, None),
        P(),
        P(None, TP),
        P(SP, None),
        P(SP, None),
        P(None, TP),
        P(TP),
        P(TP),
        P(TP, SP),
    )
    out_specs = P(SP + TP, None)
    return jax.shard_map(body, mesh=mesh, in_specs=in_specs, out_specs=out_specs, check_vma=False)
```

```python
import functools

import jax
import jax.numpy as jnp
import numpy as np
from jax import lax
from jax.experimental import pallas as pl
from jax.experimental.pallas import tpu as pltpu
from jax.sharding import Mesh
from jax.sharding import PartitionSpec as P

HEAD = 64
WINDOW = 128
QB = 128
LANES = 128
ROWS = 256
KV_ROWS = 512
EDGE = 16
POOL_SPANS = (2, 4, 8, 16)
NEG_BIG = -1e30
SP = ("z", "y")
TP = ("x", "c")
INTERPRET = False


def from_everyone(x, axis):
    peers = lax.axis_size(axis)
    return lax.all_to_all(jnp.broadcast_to(x[None], (peers, *x.shape)), axis, 0, 0, tiled=True)


def swapped(piece):
    side, depth = lax.axis_size("z"), lax.axis_size("y")
    place = lambda z, y, t: (z * depth + y) * side + t
    pairs = [
        (place(z, y, t), place(t, y, z))
        for z in range(side)
        for y in range(depth)
        for t in range(side)
    ]
    return lax.ppermute(piece, SP + TP, pairs)


def three_parts(x):
    high = lax.reduce_precision(x, 8, 7)
    middle = lax.reduce_precision(x - high, 8, 7)
    low = x - high - middle
    return jnp.concatenate([high, middle, low], axis=0).astype(jnp.bfloat16)


def rope_tables(offset, rows):
    half = HEAD // 2
    places = jnp.arange(LANES)
    inverse = 10000.0 ** (-(places % half).astype(jnp.float32) / half)
    starts = (offset + QB * jnp.arange(rows // QB)).astype(jnp.float32)
    coarse = starts[:, None] * inverse[None, :]
    sign = np.where(np.arange(LANES) % HEAD < half, -1.0, 1.0)
    exact = np.tile(10000.0 ** (-np.arange(half) / half), 4)
    fine = np.arange(QB)[:, None] * exact[None, :]
    fine = jnp.asarray(np.stack([np.cos(fine), np.sin(fine) * sign]), jnp.float32)
    sine = jnp.sin(coarse)
    return jnp.cos(coarse), jnp.where(places % HEAD < half, -sine, sine), fine


def turned(x, cosine, sine, fine, first_block):
    cosines, sines = [], []
    for block in range(x.shape[0] // QB):
        c, s = cosine[pl.ds(first_block + block, 1), :], sine[pl.ds(first_block + block, 1), :]
        cosines.append(c * fine[0] - s * fine[1])
        sines.append(s * fine[0] + c * fine[1])
    lane = lax.broadcasted_iota(jnp.int32, x.shape, 1)
    half = HEAD // 2
    other = jnp.where(lane % HEAD < half, pltpu.roll(x, LANES - half, 1), pltpu.roll(x, half, 1))
    return x * jnp.concatenate(cosines, axis=0) + other * jnp.concatenate(sines, axis=0)


def project(tokens, gain, own, other, cosine, sine, fine, normed_out, q_out, pool_out, weights):
    core = lax.axis_index("c")
    for place in range(2):

        @pl.when((pl.program_id(0) == 0) & (core == place))
        def _():
            for source, head in ((own, place), (other, 1 - place)):
                weights[head * HEAD : (head + 1) * HEAD] = source[:HEAD]
                weights[LANES + head * HEAD : LANES + (head + 1) * HEAD] = source[HEAD:LANES]

    values = tokens[...].astype(jnp.float32)
    center = jnp.mean(values, axis=-1, keepdims=True)
    values = values - center
    spread = jnp.mean(values * values, axis=-1, keepdims=True)
    normed = (values * lax.rsqrt(spread + 1e-06) * gain[...]).astype(jnp.bfloat16)
    normed_out[...] = normed
    sums = lax.dot_general(
        normed, weights[...], (((1,), (1,)), ((), ())), preferred_element_type=jnp.float32
    )
    first_block = pl.program_id(0) * (ROWS // QB)
    query = turned(sums[:, :LANES], cosine, sine, fine, first_block)
    q_out[...] = (query * HEAD ** (-0.5)).astype(jnp.bfloat16)
    pool_out[...] = sums[:, LANES:].astype(jnp.bfloat16)


def project_kv(normed, pool, ex, cosine, sine, fine, kv_out, send):
    core, step, rows = lax.axis_index("c"), pl.program_id(0), normed.shape[0]
    sums = jnp.dot(normed[...], ex[...].reshape(-1, LANES), preferred_element_type=jnp.float32)
    lane = lax.broadcasted_iota(jnp.int32, sums.shape, 1)
    kv = jnp.where(lane < HEAD, turned(sums, cosine, sine, fine, step * (rows // QB)), sums)
    kv = kv.astype(jnp.bfloat16)
    kv_out[...] = kv

    @pl.when((step == 0) & (core == 1))
    def _():
        send[:QB] = kv[:QB]
        send[QB:] = pool[:EDGE]

    @pl.when((step == pl.num_programs(0) - 1) & (core == 0))
    def _():
        send[:QB] = kv[rows - QB :]
        send[QB:] = pool[rows - EDGE :]


def mix(inner, own, other, q, kv, pool, *rest):
    out, kv_wide, pool_wide, both, sems = rest[-5:]
    core, group = lax.axis_index("c"), lax.axis_index("x")
    rows = q.shape[0]
    blocks_total = lax.axis_size(SP) * (rows // QB)
    first_block = lax.axis_index(SP) * (rows // QB)
    mine = jnp.sum(own[:3, :LANES].astype(jnp.float32), axis=0, keepdims=True)
    theirs = jnp.sum(other[:3, :LANES].astype(jnp.float32), axis=0, keepdims=True)
    first = jnp.where(core == 0, mine, theirs)
    second = jnp.where(core == 0, theirs, mine)
    scale = jnp.concatenate([first[:, :HEAD], second[:, :HEAD]], axis=1)
    kv_wide[pl.ds(pl.multiple_of((1 - core) * QB, QB), rows), :] = kv[...]
    pool_wide[EDGE : EDGE + rows, :] = pool[...].astype(jnp.float32)
    if not inner:
        halo = rest[0]
        kv_wide[pl.ds(pl.multiple_of(core * rows, QB), QB), :] = halo[:QB, :]
        edge = halo[QB:, :].astype(jnp.float32)
        pool_wide[:EDGE, :] = edge
        pool_wide[EDGE + rows :, :] = edge
    lane = lax.broadcasted_iota(jnp.int32, (QB, LANES), 1)
    row = lax.broadcasted_iota(jnp.int32, (2 * QB, 3 * QB), 0) % QB
    column = lax.broadcasted_iota(jnp.int32, (2 * QB, 3 * QB), 1)
    near = (column >= row) & (column <= row + 2 * WINDOW)
    upper = lax.broadcasted_iota(jnp.int32, (2 * QB, 1), 0) < QB
    sinks = jnp.where(upper, first[:, HEAD : HEAD + 1], second[:, HEAD : HEAD + 1])
    half = lax.shift_left(1, group)
    copies = []
    for j in range(both.shape[0]):
        i = 1 - core + j if inner else core * (rows // (2 * QB) - 1)
        start = pl.multiple_of(core * QB + 2 * QB * i, QB)
        block = first_block + core + 2 * i
        pair = q[pl.ds(start, QB), :]
        zero = jnp.zeros_like(pair)
        lower_head = jnp.where(lane < HEAD, pair, zero)
        upper_head = jnp.concatenate([pair[:, HEAD:], zero[:, HEAD:]], axis=1)
        queries = jnp.concatenate([lower_head, upper_head], axis=0)
        keys = kv_wide[pl.ds(pl.multiple_of(2 * QB * i, QB), 3 * QB), :]
        scores = lax.dot_general(
            queries, keys, (((1,), (1,)), ((), ())), preferred_element_type=jnp.float32
        )
        least = jnp.where(block == 0, QB, 0)
        limit = jnp.where(block == blocks_total - 1, 2 * QB, 3 * QB)
        valid = near & (column >= least) & (column < limit)
        scores = jnp.where(valid, scores, NEG_BIG)
        top = jnp.maximum(jnp.max(scores, axis=-1, keepdims=True), sinks)
        expo = jnp.where(valid, jnp.exp(scores - top), 0.0)
        total = jnp.sum(expo, axis=-1, keepdims=True) + jnp.exp(sinks - top)
        weights = (expo / total).astype(jnp.bfloat16)
        mixed = jnp.dot(weights, keys, preferred_element_type=jnp.float32)
        attended = jnp.concatenate([mixed[:QB, HEAD:], mixed[QB:, HEAD:]], axis=1)

        near_rows = pool_wide[pl.ds(start, QB + 2 * EDGE), :]
        size = QB + 2 * EDGE
        sums = near_rows + pltpu.roll(near_rows, 1, 0)
        chosen = sums
        for index in range(1, len(POOL_SPANS)):
            step = POOL_SPANS[index] // 4
            sums = pltpu.roll(sums, step, 0) + pltpu.roll(sums, size - step, 0)
            chosen = jnp.where(group == index, sums, chosen)
        position = block * QB + lax.broadcasted_iota(jnp.int32, (QB, 1), 0)
        counted = jnp.minimum(position + half, blocks_total * QB) - jnp.maximum(position - half, 0)
        mean = chosen[EDGE : EDGE + QB] / counted.astype(jnp.float32)
        pooled = (mean - near_rows[EDGE : EDGE + QB]) * scale
        both[j] = jnp.concatenate([attended, pooled], axis=1).astype(jnp.bfloat16)
        for peer in range(out.shape[0]):
            target = out.at[peer, pl.ds(pl.multiple_of(i * QB, QB), QB)]
            copies.append(pltpu.make_async_copy(both.at[j], target, sems.at[j, peer]))
            copies[-1].start()
    for copy in copies:
        copy.wait()


def body(tokens, norm_gain, w_query, w_key, w_value, w_pool_in, sink_logit, pool_scale, w_out):
    rows, depth = tokens.shape
    sp_count = lax.axis_size(SP)
    bf16 = jnp.bfloat16

    key_head = lax.axis_index("x") // (lax.axis_size("x") // (w_key.shape[1] // HEAD))
    key_cols = lax.dynamic_slice_in_dim(w_key, key_head * HEAD, HEAD, 1)
    value_cols = lax.dynamic_slice_in_dim(w_value, key_head * HEAD, HEAD, 1)
    exchanged = from_everyone(jnp.concatenate([key_cols, value_cols], axis=1), SP)
    peers, pieces = exchanged.shape[:2]

    out_piece = swapped(w_out.T)

    small = jnp.concatenate([pool_scale, jnp.broadcast_to(sink_logit, (HEAD,))])[None, :]
    small = three_parts(lax.optimization_barrier(small))
    small = jnp.pad(small, ((0, EDGE - 3), (0, depth - LANES)))
    own = jnp.concatenate([w_query.T, w_pool_in.T, small], axis=0)
    other = lax.ppermute(own, "c", [(0, 1), (1, 0)])

    cosine, sine, fine = rope_tables(lax.axis_index(SP) * rows, rows)

    at = lambda *shape: lambda *place: pl.BlockSpec(shape, lambda i: place)
    whole = lambda *shape: pl.BlockSpec(shape, lambda i: (0,) * len(shape))
    part = lambda *shape: pl.BlockSpec(shape, lambda i: (i,) + (0,) * (len(shape) - 1))
    shaped = lambda *shape: jax.ShapeDtypeStruct(shape, bf16)
    tables = [whole(*cosine.shape)] * 2 + [whole(*fine.shape)]
    normed, query, pool_in = pl.pallas_call(
        project,
        grid=(rows // ROWS,),
        in_specs=[part(ROWS, depth), whole(1, depth)] + [whole(*own.shape)] * 2 + tables,
        out_specs=[part(ROWS, depth), part(ROWS, LANES), part(ROWS, LANES)],
        out_shape=[shaped(rows, depth), shaped(rows, LANES), shaped(rows, LANES)],
        scratch_shapes=[pltpu.VMEM((2 * LANES, depth), bf16)],
        name="project",
        interpret=INTERPRET,
    )(tokens, norm_gain[None, :], own, other, cosine, sine, fine)
    exchanged, out_piece, normed = lax.optimization_barrier((exchanged, out_piece, normed))
    own_cols = from_everyone(out_piece, SP)
    kv, send = pl.pallas_call(
        project_kv,
        grid=(rows // KV_ROWS,),
        in_specs=[part(KV_ROWS, depth), part(KV_ROWS, LANES), whole(peers, pieces, LANES)]
        + tables,
        out_specs=[part(KV_ROWS, LANES), whole(QB + EDGE, LANES)],
        out_shape=[shaped(rows, LANES), shaped(QB + EDGE, LANES)],
        name="project_kv",
        interpret=INTERPRET,
    )(normed, pool_in, exchanged, cosine, sine, fine)

    pairs = [(2 * s, 2 * s + 2) for s in range(sp_count - 1)]
    pairs += [(2 * s + 3, 2 * s + 1) for s in range(sp_count - 1)]
    halo = lax.ppermute(send, SP + ("c",), pairs)
    peers_x = lax.axis_size("x")
    small_rows = at(EDGE, depth)(LANES // EDGE, 0)
    anywhere = pl.BlockSpec(memory_space=pl.ANY)
    local_specs = [small_rows, small_rows] + [whole(rows, LANES)] * 3

    def mixed(inner, *more):
        blocks = rows // (2 * QB) - 1 if inner else 1
        return pl.pallas_call(
            functools.partial(mix, inner),
            grid=(1,),
            in_specs=local_specs + ([] if inner else [whole(QB + EDGE, LANES), anywhere]),
            out_specs=anywhere,
            out_shape=shaped(peers_x, rows // 2, 2 * LANES),
            input_output_aliases={} if inner else {6: 0},
            scratch_shapes=[
                pltpu.VMEM((rows + QB, LANES), bf16),
                pltpu.VMEM((rows + 2 * EDGE, LANES), jnp.float32),
                pltpu.VMEM((blocks, QB, 2 * LANES), bf16),
                pltpu.SemaphoreType.DMA((blocks, peers_x)),
            ],
            name="mix_inner" if inner else "mix_outer",
            interpret=INTERPRET,
        )(own, other, query, kv, pool_in, *more)

    local = mixed(True)
    local = mixed(False, halo, local)

    local, own_cols = lax.optimization_barrier((local, own_cols))
    other_cols = lax.ppermute(own_cols, "c", [(0, 1), (1, 0)])
    joined = lax.all_to_all(local, "x", 0, 0, tiled=True)

    def matched(columns):
        columns = columns.reshape(2, peers_x, -1, LANES)
        return jnp.concatenate([columns[0], columns[1]], axis=2)

    core = lax.axis_index("c")
    mine, theirs = matched(own_cols), matched(other_cols)
    columns = jnp.concatenate(
        [jnp.where(core == 0, mine, theirs), jnp.where(core == 0, theirs, mine)], axis=1
    )
    partial_cols = jnp.einsum(
        "ptc,pnc->tn", joined, columns, preferred_element_type=jnp.float32
    ).astype(bf16)
    return lax.all_to_all(partial_cols, "x", split_axis=0, concat_axis=1, tiled=True)


def solution(mesh):
    devices = mesh.devices
    mesh = Mesh(devices.reshape(8, devices.size // 64, 4, 2), SP + TP)
    in_specs = (
        P(SP, None),
        P(),
        P(None, TP),
        P(SP, None),
        P(SP, None),
        P(None, TP),
        P(TP),
        P(TP),
        P(TP, SP),
    )
    out_specs = P(SP + TP, None)
    return jax.shard_map(body, mesh=mesh, in_specs=in_specs, out_specs=out_specs, check_vma=False)
```

```python
import functools

import jax
import jax.numpy as jnp
import numpy as np
from jax import lax
from jax.experimental import pallas as pl
from jax.experimental.pallas import tpu as pltpu
from jax.sharding import Mesh
from jax.sharding import PartitionSpec as P

HEAD = 64
WINDOW = 128
QB = 128
LANES = 128
ROWS = 256
EDGE = 16
POOL_SPANS = (2, 4, 8, 16)
NEG_BIG = -1e30
SP = ("z", "y")
TP = ("x", "c")
INTERPRET = False


def from_everyone(x, axis):
    peers = lax.axis_size(axis)
    return lax.all_to_all(jnp.broadcast_to(x[None], (peers, *x.shape)), axis, 0, 0, tiled=True)


def swapped(piece):
    side, depth = lax.axis_size("z"), lax.axis_size("y")
    place = lambda z, y, t: (z * depth + y) * side + t
    pairs = [
        (place(z, y, t), place(t, y, z))
        for z in range(side)
        for y in range(depth)
        for t in range(side)
    ]
    return lax.ppermute(piece, SP + TP, pairs)


def three_parts(x):
    high = lax.reduce_precision(x, 8, 7)
    middle = lax.reduce_precision(x - high, 8, 7)
    low = x - high - middle
    return jnp.concatenate([high, middle, low], axis=0).astype(jnp.bfloat16)


def rope_tables(offset, rows):
    half = HEAD // 2
    places = jnp.arange(LANES)
    inverse = 10000.0 ** (-(places % half).astype(jnp.float32) / half)
    starts = (offset + QB * jnp.arange(rows // QB)).astype(jnp.float32)
    coarse = starts[:, None] * inverse[None, :]
    sign = np.where(np.arange(LANES) % HEAD < half, -1.0, 1.0)
    exact = np.tile(10000.0 ** (-np.arange(half) / half), 4)
    fine = np.arange(QB)[:, None] * exact[None, :]
    fine = jnp.asarray(np.stack([np.cos(fine), np.sin(fine) * sign]), jnp.float32)
    sine = jnp.sin(coarse)
    return jnp.cos(coarse), jnp.where(places % HEAD < half, -sine, sine), fine


def turned(x, cosine, sine, fine, first_block):
    cosines, sines = [], []
    for block in range(x.shape[0] // QB):
        c, s = cosine[pl.ds(first_block + block, 1), :], sine[pl.ds(first_block + block, 1), :]
        cosines.append(c * fine[0] - s * fine[1])
        sines.append(s * fine[0] + c * fine[1])
    lane = lax.broadcasted_iota(jnp.int32, x.shape, 1)
    half = HEAD // 2
    other = jnp.where(lane % HEAD < half, pltpu.roll(x, LANES - half, 1), pltpu.roll(x, half, 1))
    return x * jnp.concatenate(cosines, axis=0) + other * jnp.concatenate(sines, axis=0)


def project(tokens, gain, own, other, cosine, sine, fine, kept, sent, q_out, pool_out, weights):
    core = lax.axis_index("c")
    for place in range(2):

        @pl.when((pl.program_id(0) == 0) & (core == place))
        def _():
            for source, head in ((own, place), (other, 1 - place)):
                weights[head * HEAD : (head + 1) * HEAD] = source[:HEAD]
                weights[LANES + head * HEAD : LANES + (head + 1) * HEAD] = source[HEAD:LANES]

    values = tokens[...].astype(jnp.float32)
    center = jnp.mean(values, axis=-1, keepdims=True)
    values = values - center
    spread = jnp.mean(values * values, axis=-1, keepdims=True)
    normed = (values * lax.rsqrt(spread + 1e-06) * gain[...]).astype(jnp.bfloat16)
    step, half = pl.program_id(0), pl.num_programs(0) // 2

    @pl.when(step < half)
    def _():
        kept[pl.ds(pl.multiple_of(step * ROWS, ROWS), ROWS), :] = normed

    @pl.when(step >= half)
    def _():
        sent[...] = normed

    sums = lax.dot_general(
        normed, weights[...], (((1,), (1,)), ((), ())), preferred_element_type=jnp.float32
    )
    first_block = pl.program_id(0) * (ROWS // QB)
    query = turned(sums[:, :LANES], cosine, sine, fine, first_block)
    q_out[...] = (query * HEAD ** (-0.5)).astype(jnp.bfloat16)
    pool_out[...] = sums[:, LANES:].astype(jnp.bfloat16)


def project_kv(kept, sent, pool, ex, cosine, sine, fine, kv_out, send, landed, sem):
    core, rows = lax.axis_index("c"), kept.shape[0]
    copy = pltpu.make_async_copy(sent, landed, sem)
    copy.start()
    weights = ex[...].reshape(-1, LANES)

    def product(normed, first_block):
        sums = jnp.dot(normed, weights, preferred_element_type=jnp.float32)
        lane = lax.broadcasted_iota(jnp.int32, sums.shape, 1)
        kv = jnp.where(lane < HEAD, turned(sums, cosine, sine, fine, first_block), sums)
        return kv.astype(jnp.bfloat16)

    lower = product(kept[...], 0)
    kv_out[:rows] = lower
    copy.wait()
    upper = product(landed[...], rows // QB)
    kv_out[rows:] = upper
    send[:QB] = jnp.where(core == 0, upper[rows - QB :], lower[:QB])
    send[QB:] = jnp.where(core == 0, pool[2 * rows - EDGE :], pool[:EDGE])


def mix(inner, own, other, q, kv, pool, *rest):
    out, kv_wide, pool_wide, both, sems = rest[-5:]
    core, group = lax.axis_index("c"), lax.axis_index("x")
    rows = q.shape[0]
    blocks_total = lax.axis_size(SP) * (rows // QB)
    first_block = lax.axis_index(SP) * (rows // QB)
    mine = jnp.sum(own[:3, :LANES].astype(jnp.float32), axis=0, keepdims=True)
    theirs = jnp.sum(other[:3, :LANES].astype(jnp.float32), axis=0, keepdims=True)
    first = jnp.where(core == 0, mine, theirs)
    second = jnp.where(core == 0, theirs, mine)
    scale = jnp.concatenate([first[:, :HEAD], second[:, :HEAD]], axis=1)
    kv_wide[pl.ds(pl.multiple_of((1 - core) * QB, QB), rows), :] = kv[...]
    pool_wide[EDGE : EDGE + rows, :] = pool[...].astype(jnp.float32)
    if not inner:
        halo = rest[0]
        kv_wide[pl.ds(pl.multiple_of(core * rows, QB), QB), :] = halo[:QB, :]
        edge = halo[QB:, :].astype(jnp.float32)
        pool_wide[:EDGE, :] = edge
        pool_wide[EDGE + rows :, :] = edge
    lane = lax.broadcasted_iota(jnp.int32, (QB, LANES), 1)
    row = lax.broadcasted_iota(jnp.int32, (2 * QB, 3 * QB), 0) % QB
    column = lax.broadcasted_iota(jnp.int32, (2 * QB, 3 * QB), 1)
    near = (column >= row) & (column <= row + 2 * WINDOW)
    upper = lax.broadcasted_iota(jnp.int32, (2 * QB, 1), 0) < QB
    sinks = jnp.where(upper, first[:, HEAD : HEAD + 1], second[:, HEAD : HEAD + 1])
    half = lax.shift_left(1, group)
    copies = []
    for j in range(both.shape[0]):
        i = 1 - core + j if inner else core * (rows // (2 * QB) - 1)
        start = pl.multiple_of(core * QB + 2 * QB * i, QB)
        block = first_block + core + 2 * i
        pair = q[pl.ds(start, QB), :]
        zero = jnp.zeros_like(pair)
        lower_head = jnp.where(lane < HEAD, pair, zero)
        upper_head = jnp.concatenate([pair[:, HEAD:], zero[:, HEAD:]], axis=1)
        queries = jnp.concatenate([lower_head, upper_head], axis=0)
        keys = kv_wide[pl.ds(pl.multiple_of(2 * QB * i, QB), 3 * QB), :]
        scores = lax.dot_general(
            queries, keys, (((1,), (1,)), ((), ())), preferred_element_type=jnp.float32
        )
        least = jnp.where(block == 0, QB, 0)
        limit = jnp.where(block == blocks_total - 1, 2 * QB, 3 * QB)
        valid = near & (column >= least) & (column < limit)
        scores = jnp.where(valid, scores, NEG_BIG)
        top = jnp.maximum(jnp.max(scores, axis=-1, keepdims=True), sinks)
        expo = jnp.where(valid, jnp.exp(scores - top), 0.0)
        total = jnp.sum(expo, axis=-1, keepdims=True) + jnp.exp(sinks - top)
        weights = (expo / total).astype(jnp.bfloat16)
        mixed = jnp.dot(weights, keys, preferred_element_type=jnp.float32)
        attended = jnp.concatenate([mixed[:QB, HEAD:], mixed[QB:, HEAD:]], axis=1)

        near_rows = pool_wide[pl.ds(start, QB + 2 * EDGE), :]
        size = QB + 2 * EDGE
        sums = near_rows + pltpu.roll(near_rows, 1, 0)
        chosen = sums
        for index in range(1, len(POOL_SPANS)):
            step = POOL_SPANS[index] // 4
            sums = pltpu.roll(sums, step, 0) + pltpu.roll(sums, size - step, 0)
            chosen = jnp.where(group == index, sums, chosen)
        position = block * QB + lax.broadcasted_iota(jnp.int32, (QB, 1), 0)
        counted = jnp.minimum(position + half, blocks_total * QB) - jnp.maximum(position - half, 0)
        mean = chosen[EDGE : EDGE + QB] / counted.astype(jnp.float32)
        pooled = (mean - near_rows[EDGE : EDGE + QB]) * scale
        both[j] = jnp.concatenate([attended, pooled], axis=1).astype(jnp.bfloat16)
        for peer in range(out.shape[0]):
            target = out.at[peer, pl.ds(pl.multiple_of(i * QB, QB), QB)]
            copies.append(pltpu.make_async_copy(both.at[j], target, sems.at[j, peer]))
            copies[-1].start()
    for copy in copies:
        copy.wait()


def body(tokens, norm_gain, w_query, w_key, w_value, w_pool_in, sink_logit, pool_scale, w_out):
    rows, depth = tokens.shape
    sp_count = lax.axis_size(SP)
    bf16 = jnp.bfloat16

    key_head = lax.axis_index("x") // (lax.axis_size("x") // (w_key.shape[1] // HEAD))
    key_cols = lax.dynamic_slice_in_dim(w_key, key_head * HEAD, HEAD, 1)
    value_cols = lax.dynamic_slice_in_dim(w_value, key_head * HEAD, HEAD, 1)
    exchanged = from_everyone(jnp.concatenate([key_cols, value_cols], axis=1), SP)
    peers, pieces = exchanged.shape[:2]

    out_piece = swapped(w_out.T)

    small = jnp.concatenate([pool_scale, jnp.broadcast_to(sink_logit, (HEAD,))])[None, :]
    small = three_parts(lax.optimization_barrier(small))
    small = jnp.pad(small, ((0, EDGE - 3), (0, depth - LANES)))
    own = jnp.concatenate([w_query.T, w_pool_in.T, small], axis=0)
    other = lax.ppermute(own, "c", [(0, 1), (1, 0)])

    cosine, sine, fine = rope_tables(lax.axis_index(SP) * rows, rows)

    at = lambda *shape: lambda *place: pl.BlockSpec(shape, lambda i: place)
    whole = lambda *shape: pl.BlockSpec(shape, lambda i: (0,) * len(shape))
    part = lambda *shape: pl.BlockSpec(shape, lambda i: (i,) + (0,) * (len(shape) - 1))
    shaped = lambda *shape: jax.ShapeDtypeStruct(shape, bf16)
    tables = [whole(*cosine.shape)] * 2 + [whole(*fine.shape)]
    on_chip = shaped(rows // 2, depth) if INTERPRET else pltpu.VMEM((rows // 2, depth), bf16)
    kept, sent, query, pool_in = pl.pallas_call(
        project,
        grid=(rows // ROWS,),
        in_specs=[part(ROWS, depth), whole(1, depth)] + [whole(*own.shape)] * 2 + tables,
        out_specs=[
            pl.BlockSpec(memory_space=pltpu.VMEM),
            pl.BlockSpec((ROWS, depth), lambda i: (jnp.maximum(i - rows // ROWS // 2, 0), 0)),
            part(ROWS, LANES),
            part(ROWS, LANES),
        ],
        out_shape=[on_chip, shaped(rows // 2, depth), shaped(rows, LANES), shaped(rows, LANES)],
        scratch_shapes=[pltpu.VMEM((2 * LANES, depth), bf16)],
        name="project",
        interpret=INTERPRET,
    )(tokens, norm_gain[None, :], own, other, cosine, sine, fine)
    exchanged, out_piece, sent = lax.optimization_barrier((exchanged, out_piece, sent))
    own_cols = from_everyone(out_piece, SP)
    kv, send = pl.pallas_call(
        project_kv,
        grid=(1,),
        in_specs=[
            pl.BlockSpec(memory_space=pltpu.VMEM),
            pl.BlockSpec(memory_space=pl.ANY),
            whole(rows, LANES),
            whole(peers, pieces, LANES),
        ]
        + tables,
        out_specs=[whole(rows, LANES), whole(QB + EDGE, LANES)],
        out_shape=[shaped(rows, LANES), shaped(QB + EDGE, LANES)],
        scratch_shapes=[pltpu.VMEM((rows // 2, depth), bf16), pltpu.SemaphoreType.DMA],
        name="project_kv",
        interpret=INTERPRET,
    )(kept, sent, pool_in, exchanged, cosine, sine, fine)

    pairs = [(2 * s, 2 * s + 2) for s in range(sp_count - 1)]
    pairs += [(2 * s + 3, 2 * s + 1) for s in range(sp_count - 1)]
    halo = lax.ppermute(send, SP + ("c",), pairs)
    peers_x = lax.axis_size("x")
    small_rows = at(EDGE, depth)(LANES // EDGE, 0)
    anywhere = pl.BlockSpec(memory_space=pl.ANY)
    local_specs = [small_rows, small_rows] + [whole(rows, LANES)] * 3

    def mixed(inner, *more):
        blocks = rows // (2 * QB) - 1 if inner else 1
        return pl.pallas_call(
            functools.partial(mix, inner),
            grid=(1,),
            in_specs=local_specs + ([] if inner else [whole(QB + EDGE, LANES), anywhere]),
            out_specs=anywhere,
            out_shape=shaped(peers_x, rows // 2, 2 * LANES),
            input_output_aliases={} if inner else {6: 0},
            scratch_shapes=[
                pltpu.VMEM((rows + QB, LANES), bf16),
                pltpu.VMEM((rows + 2 * EDGE, LANES), jnp.float32),
                pltpu.VMEM((blocks, QB, 2 * LANES), bf16),
                pltpu.SemaphoreType.DMA((blocks, peers_x)),
            ],
            name="mix_inner" if inner else "mix_outer",
            interpret=INTERPRET,
        )(own, other, query, kv, pool_in, *more)

    local = mixed(True)
    local = mixed(False, halo, local)

    local, own_cols = lax.optimization_barrier((local, own_cols))
    other_cols = lax.ppermute(own_cols, "c", [(0, 1), (1, 0)])
    joined = lax.all_to_all(local, "x", 0, 0, tiled=True)

    def matched(columns):
        columns = columns.reshape(2, peers_x, -1, LANES)
        return jnp.concatenate([columns[0], columns[1]], axis=2)

    core = lax.axis_index("c")
    mine, theirs = matched(own_cols), matched(other_cols)
    columns = jnp.concatenate(
        [jnp.where(core == 0, mine, theirs), jnp.where(core == 0, theirs, mine)], axis=1
    )
    partial_cols = jnp.einsum(
        "ptc,pnc->tn", joined, columns, preferred_element_type=jnp.float32
    ).astype(bf16)
    return lax.all_to_all(partial_cols, "x", split_axis=0, concat_axis=1, tiled=True)


def solution(mesh):
    devices = mesh.devices
    mesh = Mesh(devices.reshape(8, devices.size // 64, 4, 2), SP + TP)
    in_specs = (
        P(SP, None),
        P(),
        P(None, TP),
        P(SP, None),
        P(SP, None),
        P(None, TP),
        P(TP),
        P(TP),
        P(TP, SP),
    )
    out_specs = P(SP + TP, None)
    return jax.shard_map(body, mesh=mesh, in_specs=in_specs, out_specs=out_specs, check_vma=False)
```

```python
import functools

import jax
import jax.numpy as jnp
import numpy as np
from jax import lax
from jax.experimental import pallas as pl
from jax.experimental.pallas import tpu as pltpu
from jax.sharding import Mesh
from jax.sharding import PartitionSpec as P

HEAD = 64
WINDOW = 128
QB = 128
LANES = 128
ROWS = 256
KV_ROWS = 512
EDGE = 16
POOL_SPANS = (2, 4, 8, 16)
NEG_BIG = -1e30
SP = ("z", "y")
TP = ("x", "c")
INTERPRET = False


def from_everyone(x, axis):
    peers = lax.axis_size(axis)
    return lax.all_to_all(jnp.broadcast_to(x[None], (peers, *x.shape)), axis, 0, 0, tiled=True)


def swapped(piece):
    side, depth = lax.axis_size("z"), lax.axis_size("y")
    place = lambda z, y, t: (z * depth + y) * side + t
    pairs = [
        (place(z, y, t), place(t, y, z))
        for z in range(side)
        for y in range(depth)
        for t in range(side)
    ]
    return lax.ppermute(piece, SP + TP, pairs)


def on_chip(x):
    return x if INTERPRET else pltpu.with_memory_space_constraint(x, pltpu.VMEM)


def three_parts(x):
    high = lax.reduce_precision(x, 8, 7)
    middle = lax.reduce_precision(x - high, 8, 7)
    low = x - high - middle
    return jnp.concatenate([high, middle, low], axis=0).astype(jnp.bfloat16)


def rope_tables(offset, rows):
    half = HEAD // 2
    places = jnp.arange(LANES)
    inverse = 10000.0 ** (-(places % half).astype(jnp.float32) / half)
    starts = (offset + QB * jnp.arange(rows // QB)).astype(jnp.float32)
    coarse = starts[:, None] * inverse[None, :]
    sign = np.where(np.arange(LANES) % HEAD < half, -1.0, 1.0)
    exact = np.tile(10000.0 ** (-np.arange(half) / half), 4)
    fine = np.arange(QB)[:, None] * exact[None, :]
    fine = jnp.asarray(np.stack([np.cos(fine), np.sin(fine) * sign]), jnp.float32)
    sine = jnp.sin(coarse)
    return jnp.cos(coarse), jnp.where(places % HEAD < half, -sine, sine), fine


def turned(x, cosine, sine, fine, first_block):
    cosines, sines = [], []
    for block in range(x.shape[0] // QB):
        c, s = cosine[pl.ds(first_block + block, 1), :], sine[pl.ds(first_block + block, 1), :]
        cosines.append(c * fine[0] - s * fine[1])
        sines.append(s * fine[0] + c * fine[1])
    lane = lax.broadcasted_iota(jnp.int32, x.shape, 1)
    half = HEAD // 2
    other = jnp.where(lane % HEAD < half, pltpu.roll(x, LANES - half, 1), pltpu.roll(x, half, 1))
    return x * jnp.concatenate(cosines, axis=0) + other * jnp.concatenate(sines, axis=0)


def project(tokens, gain, own, other, cosine, sine, fine, normed_out, q_out, pool_out, parts, weights):
    core = lax.axis_index("c")
    for place in range(2):

        @pl.when((pl.program_id(0) == 0) & (core == place))
        def _():
            for source, head in ((own, place), (other, 1 - place)):
                weights[head * HEAD : (head + 1) * HEAD] = source[:HEAD]
                weights[LANES + head * HEAD : LANES + (head + 1) * HEAD] = source[HEAD:LANES]
                parts[head * EDGE : (head + 1) * EDGE] = source[LANES:, :LANES]

    values = tokens[...].astype(jnp.float32)
    center = jnp.mean(values, axis=-1, keepdims=True)
    values = values - center
    spread = jnp.mean(values * values, axis=-1, keepdims=True)
    normed = (values * lax.rsqrt(spread + 1e-06) * gain[...]).astype(jnp.bfloat16)
    normed_out[...] = normed
    sums = lax.dot_general(
        normed, weights[...], (((1,), (1,)), ((), ())), preferred_element_type=jnp.float32
    )
    first_block = pl.program_id(0) * (ROWS // QB)
    query = turned(sums[:, :LANES], cosine, sine, fine, first_block)
    q_out[...] = (query * HEAD ** (-0.5)).astype(jnp.bfloat16)
    pool_out[...] = sums[:, LANES:].astype(jnp.bfloat16)


def project_kv(normed, pool, ex, cosine, sine, fine, kv_out, send):
    core, step, rows = lax.axis_index("c"), pl.program_id(0), normed.shape[0]
    sums = jnp.dot(normed[...], ex[...].reshape(-1, LANES), preferred_element_type=jnp.float32)
    lane = lax.broadcasted_iota(jnp.int32, sums.shape, 1)
    kv = jnp.where(lane < HEAD, turned(sums, cosine, sine, fine, step * (rows // QB)), sums)
    kv = kv.astype(jnp.bfloat16)
    kv_out[...] = kv

    @pl.when((step == 0) & (core == 1))
    def _():
        send[:QB] = kv[:QB]
        send[QB:] = pool[:EDGE]

    @pl.when((step == pl.num_programs(0) - 1) & (core == 0))
    def _():
        send[:QB] = kv[rows - QB :]
        send[QB:] = pool[rows - EDGE :]


def mix(inner, parts, q, kv, pool, *rest):
    out, kv_wide, pool_wide, both, sems = rest[-5:]
    core, group = lax.axis_index("c"), lax.axis_index("x")
    rows = q.shape[0]
    blocks_total = lax.axis_size(SP) * (rows // QB)
    first_block = lax.axis_index(SP) * (rows // QB)
    first = jnp.sum(parts[:3].astype(jnp.float32), axis=0, keepdims=True)
    second = jnp.sum(parts[EDGE : EDGE + 3].astype(jnp.float32), axis=0, keepdims=True)
    scale = jnp.concatenate([first[:, :HEAD], second[:, :HEAD]], axis=1)
    kv_wide[pl.ds(pl.multiple_of((1 - core) * QB, QB), rows), :] = kv[...]
    pool_wide[EDGE : EDGE + rows, :] = pool[...].astype(jnp.float32)
    if not inner:
        halo = rest[0]
        kv_wide[pl.ds(pl.multiple_of(core * rows, QB), QB), :] = halo[:QB, :]
        edge = halo[QB:, :].astype(jnp.float32)
        pool_wide[:EDGE, :] = edge
        pool_wide[EDGE + rows :, :] = edge
    lane = lax.broadcasted_iota(jnp.int32, (QB, LANES), 1)
    row = lax.broadcasted_iota(jnp.int32, (2 * QB, 3 * QB), 0) % QB
    column = lax.broadcasted_iota(jnp.int32, (2 * QB, 3 * QB), 1)
    near = (column >= row) & (column <= row + 2 * WINDOW)
    upper = lax.broadcasted_iota(jnp.int32, (2 * QB, 1), 0) < QB
    sinks = jnp.where(upper, first[:, HEAD : HEAD + 1], second[:, HEAD : HEAD + 1])
    half = lax.shift_left(1, group)
    copies = []
    for j in range(both.shape[0]):
        i = 1 - core + j if inner else core * (rows // (2 * QB) - 1)
        start = pl.multiple_of(core * QB + 2 * QB * i, QB)
        block = first_block + core + 2 * i
        pair = q[pl.ds(start, QB), :]
        zero = jnp.zeros_like(pair)
        lower_head = jnp.where(lane < HEAD, pair, zero)
        upper_head = jnp.concatenate([pair[:, HEAD:], zero[:, HEAD:]], axis=1)
        queries = jnp.concatenate([lower_head, upper_head], axis=0)
        keys = kv_wide[pl.ds(pl.multiple_of(2 * QB * i, QB), 3 * QB), :]
        scores = lax.dot_general(
            queries, keys, (((1,), (1,)), ((), ())), preferred_element_type=jnp.float32
        )
        least = jnp.where(block == 0, QB, 0)
        limit = jnp.where(block == blocks_total - 1, 2 * QB, 3 * QB)
        valid = near & (column >= least) & (column < limit)
        scores = jnp.where(valid, scores, NEG_BIG)
        top = jnp.maximum(jnp.max(scores, axis=-1, keepdims=True), sinks)
        expo = jnp.where(valid, jnp.exp(scores - top), 0.0)
        total = jnp.sum(expo, axis=-1, keepdims=True) + jnp.exp(sinks - top)
        weights = (expo / total).astype(jnp.bfloat16)
        mixed = jnp.dot(weights, keys, preferred_element_type=jnp.float32)
        attended = jnp.concatenate([mixed[:QB, HEAD:], mixed[QB:, HEAD:]], axis=1)

        near_rows = pool_wide[pl.ds(start, QB + 2 * EDGE), :]
        size = QB + 2 * EDGE
        sums = near_rows + pltpu.roll(near_rows, 1, 0)
        chosen = sums
        for index in range(1, len(POOL_SPANS)):
            step = POOL_SPANS[index] // 4
            sums = pltpu.roll(sums, step, 0) + pltpu.roll(sums, size - step, 0)
            chosen = jnp.where(group == index, sums, chosen)
        position = block * QB + lax.broadcasted_iota(jnp.int32, (QB, 1), 0)
        counted = jnp.minimum(position + half, blocks_total * QB) - jnp.maximum(position - half, 0)
        mean = chosen[EDGE : EDGE + QB] / counted.astype(jnp.float32)
        pooled = (mean - near_rows[EDGE : EDGE + QB]) * scale
        both[j] = jnp.concatenate([attended, pooled], axis=1).astype(jnp.bfloat16)
        for peer in range(out.shape[0]):
            target = out.at[peer, pl.ds(pl.multiple_of(i * QB, QB), QB)]
            copies.append(pltpu.make_async_copy(both.at[j], target, sems.at[j, peer]))
            copies[-1].start()
    for copy in copies:
        copy.wait()


def body(tokens, norm_gain, w_query, w_key, w_value, w_pool_in, sink_logit, pool_scale, w_out):
    rows, depth = tokens.shape
    sp_count = lax.axis_size(SP)
    bf16 = jnp.bfloat16

    key_head = lax.axis_index("x") // (lax.axis_size("x") // (w_key.shape[1] // HEAD))
    key_cols = lax.dynamic_slice_in_dim(w_key, key_head * HEAD, HEAD, 1)
    value_cols = lax.dynamic_slice_in_dim(w_value, key_head * HEAD, HEAD, 1)
    exchanged = from_everyone(jnp.concatenate([key_cols, value_cols], axis=1), SP)

    out_piece = swapped(w_out.T)

    small = jnp.concatenate([pool_scale, jnp.broadcast_to(sink_logit, (HEAD,))])[None, :]
    small = three_parts(lax.optimization_barrier(small))
    small = jnp.pad(small, ((0, EDGE - 3), (0, depth - LANES)))
    own = jnp.concatenate([w_query.T, w_pool_in.T, small], axis=0)
    other = lax.ppermute(own, "c", [(0, 1), (1, 0)])

    cosine, sine, fine = rope_tables(lax.axis_index(SP) * rows, rows)

    held = pl.BlockSpec(memory_space=pltpu.VMEM)
    whole = lambda *shape: pl.BlockSpec(shape, lambda i: (0,) * len(shape))
    part = lambda *shape: pl.BlockSpec(shape, lambda i: (i,) + (0,) * (len(shape) - 1))
    shaped = lambda *shape: jax.ShapeDtypeStruct(shape, bf16)
    tables = [whole(*cosine.shape)] * 2 + [whole(*fine.shape)]
    normed, query, pool_in, parts = pl.pallas_call(
        project,
        grid=(rows // ROWS,),
        in_specs=[part(ROWS, depth), whole(1, depth)] + [held] * 2 + tables,
        out_specs=[part(ROWS, depth)] + [part(ROWS, LANES)] * 2 + [whole(2 * EDGE, LANES)],
        out_shape=[shaped(rows, depth)]
        + [shaped(rows, LANES)] * 2
        + [shaped(2 * EDGE, LANES)],
        scratch_shapes=[pltpu.VMEM((2 * LANES, depth), bf16)],
        name="project",
        interpret=INTERPRET,
    )(tokens, norm_gain[None, :], on_chip(own), on_chip(other), cosine, sine, fine)
    exchanged, out_piece, normed = lax.optimization_barrier((exchanged, out_piece, normed))
    own_cols = from_everyone(out_piece, SP)
    kv, send = pl.pallas_call(
        project_kv,
        grid=(rows // KV_ROWS,),
        in_specs=[part(KV_ROWS, depth), part(KV_ROWS, LANES), held]
        + tables,
        out_specs=[part(KV_ROWS, LANES), whole(QB + EDGE, LANES)],
        out_shape=[shaped(rows, LANES), shaped(QB + EDGE, LANES)],
        name="project_kv",
        interpret=INTERPRET,
    )(normed, pool_in, on_chip(exchanged), cosine, sine, fine)

    pairs = [(2 * s, 2 * s + 2) for s in range(sp_count - 1)]
    pairs += [(2 * s + 3, 2 * s + 1) for s in range(sp_count - 1)]
    halo = lax.ppermute(send, SP + ("c",), pairs)
    peers_x = lax.axis_size("x")
    anywhere = pl.BlockSpec(memory_space=pl.ANY)
    local_specs = [whole(2 * EDGE, LANES)] + [whole(rows, LANES)] * 3

    def mixed(inner, *more):
        blocks = rows // (2 * QB) - 1 if inner else 1
        return pl.pallas_call(
            functools.partial(mix, inner),
            grid=(1,),
            in_specs=local_specs + ([] if inner else [held, anywhere]),
            out_specs=anywhere,
            out_shape=shaped(peers_x, rows // 2, 2 * LANES),
            input_output_aliases={} if inner else {5: 0},
            scratch_shapes=[
                pltpu.VMEM((rows + QB, LANES), bf16),
                pltpu.VMEM((rows + 2 * EDGE, LANES), jnp.float32),
                pltpu.VMEM((blocks, QB, 2 * LANES), bf16),
                pltpu.SemaphoreType.DMA((blocks, peers_x)),
            ],
            name="mix_inner" if inner else "mix_outer",
            interpret=INTERPRET,
        )(parts, query, kv, pool_in, *more)

    local = mixed(True)
    local = mixed(False, on_chip(halo), local)

    local, own_cols = lax.optimization_barrier((local, own_cols))
    other_cols = lax.ppermute(own_cols, "c", [(0, 1), (1, 0)])
    joined = lax.all_to_all(local, "x", 0, 0, tiled=True)

    def matched(columns):
        columns = columns.reshape(2, peers_x, -1, LANES)
        return jnp.concatenate([columns[0], columns[1]], axis=2)

    core = lax.axis_index("c")
    mine, theirs = matched(own_cols), matched(other_cols)
    columns = jnp.concatenate(
        [jnp.where(core == 0, mine, theirs), jnp.where(core == 0, theirs, mine)], axis=1
    )
    partial_cols = jnp.einsum(
        "ptc,pnc->tn", joined, columns, preferred_element_type=jnp.float32
    ).astype(bf16)
    return lax.all_to_all(partial_cols, "x", split_axis=0, concat_axis=1, tiled=True)


def solution(mesh):
    devices = mesh.devices
    mesh = Mesh(devices.reshape(8, devices.size // 64, 4, 2), SP + TP)
    in_specs = (
        P(SP, None),
        P(),
        P(None, TP),
        P(SP, None),
        P(SP, None),
        P(None, TP),
        P(TP),
        P(TP),
        P(TP, SP),
    )
    out_specs = P(SP + TP, None)
    return jax.shard_map(body, mesh=mesh, in_specs=in_specs, out_specs=out_specs, check_vma=False)
```

```python
import functools

import jax
import jax.numpy as jnp
import numpy as np
from jax import lax
from jax.experimental import pallas as pl
from jax.experimental.pallas import tpu as pltpu
from jax.sharding import Mesh
from jax.sharding import PartitionSpec as P

HEAD = 64
WINDOW = 128
QB = 128
LANES = 128
ROWS = 256
KV_ROWS = 512
EDGE = 16
POOL_SPANS = (2, 4, 8, 16)
NEG_BIG = -1e30
SP = ("z", "y")
TP = ("x", "c")
INTERPRET = False


def from_everyone(x, axis):
    peers = lax.axis_size(axis)
    return lax.all_to_all(jnp.broadcast_to(x[None], (peers, *x.shape)), axis, 0, 0, tiled=True)


def swapped(piece):
    side, depth = lax.axis_size("z"), lax.axis_size("y")
    place = lambda z, y, t: (z * depth + y) * side + t
    pairs = [
        (place(z, y, t), place(t, y, z))
        for z in range(side)
        for y in range(depth)
        for t in range(side)
    ]
    return lax.ppermute(piece, SP + TP, pairs)


def on_chip(x):
    return x if INTERPRET else pltpu.with_memory_space_constraint(x, pltpu.VMEM)


def three_parts(x):
    high = lax.reduce_precision(x, 8, 7)
    middle = lax.reduce_precision(x - high, 8, 7)
    low = x - high - middle
    return jnp.concatenate([high, middle, low], axis=0).astype(jnp.bfloat16)


def rope_tables(offset, rows):
    half = HEAD // 2
    places = jnp.arange(LANES)
    inverse = 10000.0 ** (-(places % half).astype(jnp.float32) / half)
    starts = (offset + QB * jnp.arange(rows // QB)).astype(jnp.float32)
    coarse = starts[:, None] * inverse[None, :]
    sign = np.where(np.arange(LANES) % HEAD < half, -1.0, 1.0)
    exact = np.tile(10000.0 ** (-np.arange(half) / half), 4)
    fine = np.arange(QB)[:, None] * exact[None, :]
    fine = jnp.asarray(np.stack([np.cos(fine), np.sin(fine) * sign]), jnp.float32)
    sine = jnp.sin(coarse)
    return jnp.cos(coarse), jnp.where(places % HEAD < half, -sine, sine), fine


def turned(x, cosine, sine, fine, first_block):
    cosines, sines = [], []
    for block in range(x.shape[0] // QB):
        c, s = cosine[pl.ds(first_block + block, 1), :], sine[pl.ds(first_block + block, 1), :]
        cosines.append(c * fine[0] - s * fine[1])
        sines.append(s * fine[0] + c * fine[1])
    lane = lax.broadcasted_iota(jnp.int32, x.shape, 1)
    half = HEAD // 2
    other = jnp.where(lane % HEAD < half, pltpu.roll(x, LANES - half, 1), pltpu.roll(x, half, 1))
    return x * jnp.concatenate(cosines, axis=0) + other * jnp.concatenate(sines, axis=0)


def project(tokens, gain, own, other, cosine, sine, fine, normed_out, q_out, pool_out, parts, weights):
    core = lax.axis_index("c")
    for place in range(2):

        @pl.when((pl.program_id(0) == 0) & (core == place))
        def _():
            for source, head in ((own, place), (other, 1 - place)):
                weights[head * HEAD : (head + 1) * HEAD] = source[:HEAD]
                weights[LANES + head * HEAD : LANES + (head + 1) * HEAD] = source[HEAD:LANES]
                parts[head * EDGE : (head + 1) * EDGE] = source[LANES:, :LANES]

    values = tokens[...].astype(jnp.float32)
    center = jnp.mean(values, axis=-1, keepdims=True)
    values = values - center
    spread = jnp.mean(values * values, axis=-1, keepdims=True)
    normed = (values * lax.rsqrt(spread + 1e-06) * gain[...]).astype(jnp.bfloat16)
    normed_out[...] = normed
    sums = lax.dot_general(
        normed, weights[...], (((1,), (1,)), ((), ())), preferred_element_type=jnp.float32
    )
    first_block = pl.program_id(0) * (ROWS // QB)
    query = turned(sums[:, :LANES], cosine, sine, fine, first_block)
    here = pl.ds(pl.multiple_of(pl.program_id(0) * ROWS, ROWS), ROWS)
    q_out[here, :] = (query * HEAD ** (-0.5)).astype(jnp.bfloat16)
    pool_out[here, :] = sums[:, LANES:].astype(jnp.bfloat16)


def project_kv(normed, pool, ex, cosine, sine, fine, kv_out, send):
    core, step, rows = lax.axis_index("c"), pl.program_id(0), normed.shape[0]
    sums = jnp.dot(normed[...], ex[...].reshape(-1, LANES), preferred_element_type=jnp.float32)
    lane = lax.broadcasted_iota(jnp.int32, sums.shape, 1)
    kv = jnp.where(lane < HEAD, turned(sums, cosine, sine, fine, step * (rows // QB)), sums)
    kv = kv.astype(jnp.bfloat16)
    kv_out[pl.ds(pl.multiple_of(step * rows, rows), rows), :] = kv

    @pl.when((step == 0) & (core == 1))
    def _():
        send[:QB] = kv[:QB]
        send[QB:] = pool[:EDGE]

    @pl.when((step == pl.num_programs(0) - 1) & (core == 0))
    def _():
        send[:QB] = kv[rows - QB :]
        send[QB:] = pool[pool.shape[0] - EDGE :]


def mix(inner, parts, q, kv, pool, *rest):
    out, kv_wide, pool_wide, both, sems = rest[-5:]
    core, group = lax.axis_index("c"), lax.axis_index("x")
    rows = q.shape[0]
    blocks_total = lax.axis_size(SP) * (rows // QB)
    first_block = lax.axis_index(SP) * (rows // QB)
    first = jnp.sum(parts[:3].astype(jnp.float32), axis=0, keepdims=True)
    second = jnp.sum(parts[EDGE : EDGE + 3].astype(jnp.float32), axis=0, keepdims=True)
    scale = jnp.concatenate([first[:, :HEAD], second[:, :HEAD]], axis=1)
    kv_wide[pl.ds(pl.multiple_of((1 - core) * QB, QB), rows), :] = kv[...]
    pool_wide[EDGE : EDGE + rows, :] = pool[...].astype(jnp.float32)
    if not inner:
        halo = rest[0]
        kv_wide[pl.ds(pl.multiple_of(core * rows, QB), QB), :] = halo[:QB, :]
        edge = halo[QB:, :].astype(jnp.float32)
        pool_wide[:EDGE, :] = edge
        pool_wide[EDGE + rows :, :] = edge
    lane = lax.broadcasted_iota(jnp.int32, (QB, LANES), 1)
    row = lax.broadcasted_iota(jnp.int32, (2 * QB, 3 * QB), 0) % QB
    column = lax.broadcasted_iota(jnp.int32, (2 * QB, 3 * QB), 1)
    near = (column >= row) & (column <= row + 2 * WINDOW)
    upper = lax.broadcasted_iota(jnp.int32, (2 * QB, 1), 0) < QB
    sinks = jnp.where(upper, first[:, HEAD : HEAD + 1], second[:, HEAD : HEAD + 1])
    half = lax.shift_left(1, group)
    copies = []
    for j in range(both.shape[0]):
        i = 1 - core + j if inner else core * (rows // (2 * QB) - 1)
        start = pl.multiple_of(core * QB + 2 * QB * i, QB)
        block = first_block + core + 2 * i
        pair = q[pl.ds(start, QB), :]
        zero = jnp.zeros_like(pair)
        lower_head = jnp.where(lane < HEAD, pair, zero)
        upper_head = jnp.concatenate([pair[:, HEAD:], zero[:, HEAD:]], axis=1)
        queries = jnp.concatenate([lower_head, upper_head], axis=0)
        keys = kv_wide[pl.ds(pl.multiple_of(2 * QB * i, QB), 3 * QB), :]
        scores = lax.dot_general(
            queries, keys, (((1,), (1,)), ((), ())), preferred_element_type=jnp.float32
        )
        least = jnp.where(block == 0, QB, 0)
        limit = jnp.where(block == blocks_total - 1, 2 * QB, 3 * QB)
        valid = near & (column >= least) & (column < limit)
        scores = jnp.where(valid, scores, NEG_BIG)
        top = jnp.maximum(jnp.max(scores, axis=-1, keepdims=True), sinks)
        expo = jnp.where(valid, jnp.exp(scores - top), 0.0)
        total = jnp.sum(expo, axis=-1, keepdims=True) + jnp.exp(sinks - top)
        weights = (expo / total).astype(jnp.bfloat16)
        mixed = jnp.dot(weights, keys, preferred_element_type=jnp.float32)
        attended = jnp.concatenate([mixed[:QB, HEAD:], mixed[QB:, HEAD:]], axis=1)

        near_rows = pool_wide[pl.ds(start, QB + 2 * EDGE), :]
        size = QB + 2 * EDGE
        sums = near_rows + pltpu.roll(near_rows, 1, 0)
        chosen = sums
        for index in range(1, len(POOL_SPANS)):
            step = POOL_SPANS[index] // 4
            sums = pltpu.roll(sums, step, 0) + pltpu.roll(sums, size - step, 0)
            chosen = jnp.where(group == index, sums, chosen)
        position = block * QB + lax.broadcasted_iota(jnp.int32, (QB, 1), 0)
        counted = jnp.minimum(position + half, blocks_total * QB) - jnp.maximum(position - half, 0)
        mean = chosen[EDGE : EDGE + QB] / counted.astype(jnp.float32)
        pooled = (mean - near_rows[EDGE : EDGE + QB]) * scale
        both[j] = jnp.concatenate([attended, pooled], axis=1).astype(jnp.bfloat16)
        for peer in range(out.shape[0]):
            target = out.at[peer, pl.ds(pl.multiple_of(i * QB, QB), QB)]
            copies.append(pltpu.make_async_copy(both.at[j], target, sems.at[j, peer]))
            copies[-1].start()
    for copy in copies:
        copy.wait()


def body(tokens, norm_gain, w_query, w_key, w_value, w_pool_in, sink_logit, pool_scale, w_out):
    rows, depth = tokens.shape
    sp_count = lax.axis_size(SP)
    bf16 = jnp.bfloat16

    key_head = lax.axis_index("x") // (lax.axis_size("x") // (w_key.shape[1] // HEAD))
    key_cols = lax.dynamic_slice_in_dim(w_key, key_head * HEAD, HEAD, 1)
    value_cols = lax.dynamic_slice_in_dim(w_value, key_head * HEAD, HEAD, 1)
    exchanged = from_everyone(jnp.concatenate([key_cols, value_cols], axis=1), SP)

    out_piece = swapped(w_out.T)

    small = jnp.concatenate([pool_scale, jnp.broadcast_to(sink_logit, (HEAD,))])[None, :]
    small = three_parts(lax.optimization_barrier(small))
    small = jnp.pad(small, ((0, EDGE - 3), (0, depth - LANES)))
    own = jnp.concatenate([w_query.T, w_pool_in.T, small], axis=0)
    other = lax.ppermute(own, "c", [(0, 1), (1, 0)])

    cosine, sine, fine = rope_tables(lax.axis_index(SP) * rows, rows)

    held = pl.BlockSpec(memory_space=pltpu.VMEM)
    whole = lambda *shape: pl.BlockSpec(shape, lambda i: (0,) * len(shape))
    part = lambda *shape: pl.BlockSpec(shape, lambda i: (i,) + (0,) * (len(shape) - 1))
    shaped = lambda *shape: jax.ShapeDtypeStruct(shape, bf16)
    kept = lambda *shape: shaped(*shape) if INTERPRET else pltpu.VMEM(shape, bf16)
    tables = [whole(*cosine.shape)] * 2 + [whole(*fine.shape)]
    normed, query, pool_in, parts = pl.pallas_call(
        project,
        grid=(rows // ROWS,),
        in_specs=[part(ROWS, depth), whole(1, depth)] + [held] * 2 + tables,
        out_specs=[part(ROWS, depth)] + [held] * 3,
        out_shape=[shaped(rows, depth)]
        + [kept(rows, LANES)] * 2
        + [kept(2 * EDGE, LANES)],
        scratch_shapes=[pltpu.VMEM((2 * LANES, depth), bf16)],
        name="project",
        interpret=INTERPRET,
    )(tokens, norm_gain[None, :], on_chip(own), on_chip(other), cosine, sine, fine)
    exchanged, out_piece, normed = lax.optimization_barrier((exchanged, out_piece, normed))
    own_cols = from_everyone(out_piece, SP)
    kv, send = pl.pallas_call(
        project_kv,
        grid=(rows // KV_ROWS,),
        in_specs=[part(KV_ROWS, depth), held, held]
        + tables,
        out_specs=[held, held],
        out_shape=[kept(rows, LANES), kept(QB + EDGE, LANES)],
        name="project_kv",
        interpret=INTERPRET,
    )(normed, on_chip(pool_in), on_chip(exchanged), cosine, sine, fine)

    pairs = [(2 * s, 2 * s + 2) for s in range(sp_count - 1)]
    pairs += [(2 * s + 3, 2 * s + 1) for s in range(sp_count - 1)]
    halo = lax.ppermute(send, SP + ("c",), pairs)
    peers_x = lax.axis_size("x")
    anywhere = pl.BlockSpec(memory_space=pl.ANY)
    local_specs = [held] * 4

    def mixed(inner, *more):
        blocks = rows // (2 * QB) - 1 if inner else 1
        return pl.pallas_call(
            functools.partial(mix, inner),
            grid=(1,),
            in_specs=local_specs + ([] if inner else [held, anywhere]),
            out_specs=anywhere,
            out_shape=shaped(peers_x, rows // 2, 2 * LANES),
            input_output_aliases={} if inner else {5: 0},
            scratch_shapes=[
                pltpu.VMEM((rows + QB, LANES), bf16),
                pltpu.VMEM((rows + 2 * EDGE, LANES), jnp.float32),
                pltpu.VMEM((blocks, QB, 2 * LANES), bf16),
                pltpu.SemaphoreType.DMA((blocks, peers_x)),
            ],
            name="mix_inner" if inner else "mix_outer",
            interpret=INTERPRET,
        )(on_chip(parts), on_chip(query), on_chip(kv), on_chip(pool_in), *more)

    local = mixed(True)
    local = mixed(False, on_chip(halo), local)

    local, own_cols = lax.optimization_barrier((local, own_cols))
    other_cols = lax.ppermute(own_cols, "c", [(0, 1), (1, 0)])
    joined = lax.all_to_all(local, "x", 0, 0, tiled=True)

    def matched(columns):
        columns = columns.reshape(2, peers_x, -1, LANES)
        return jnp.concatenate([columns[0], columns[1]], axis=2)

    core = lax.axis_index("c")
    mine, theirs = matched(own_cols), matched(other_cols)
    columns = jnp.concatenate(
        [jnp.where(core == 0, mine, theirs), jnp.where(core == 0, theirs, mine)], axis=1
    )
    partial_cols = jnp.einsum(
        "ptc,pnc->tn", joined, columns, preferred_element_type=jnp.float32
    ).astype(bf16)
    return lax.all_to_all(partial_cols, "x", split_axis=0, concat_axis=1, tiled=True)


def solution(mesh):
    devices = mesh.devices
    mesh = Mesh(devices.reshape(8, devices.size // 64, 4, 2), SP + TP)
    in_specs = (
        P(SP, None),
        P(),
        P(None, TP),
        P(SP, None),
        P(SP, None),
        P(None, TP),
        P(TP),
        P(TP),
        P(TP, SP),
    )
    out_specs = P(SP + TP, None)
    return jax.shard_map(body, mesh=mesh, in_specs=in_specs, out_specs=out_specs, check_vma=False)
```

```python
import functools

import jax
import jax.numpy as jnp
import numpy as np
from jax import lax
from jax.experimental import pallas as pl
from jax.experimental.pallas import tpu as pltpu
from jax.sharding import Mesh
from jax.sharding import PartitionSpec as P

HEAD = 64
WINDOW = 128
QB = 128
LANES = 128
ROWS = 256
KV_ROWS = 512
EDGE = 16
POOL_SPANS = (2, 4, 8, 16)
NEG_BIG = -1e30
SP = ("z", "y")
TP = ("x", "c")
INTERPRET = False


def from_everyone(x, axis):
    peers = lax.axis_size(axis)
    return lax.all_to_all(jnp.broadcast_to(x[None], (peers, *x.shape)), axis, 0, 0, tiled=True)


def swapped(piece):
    side, depth = lax.axis_size("z"), lax.axis_size("y")
    place = lambda z, y, t: (z * depth + y) * side + t
    pairs = [
        (place(z, y, t), place(t, y, z))
        for z in range(side)
        for y in range(depth)
        for t in range(side)
    ]
    return lax.ppermute(piece, SP + TP, pairs)


def on_chip(x):
    return x if INTERPRET else pltpu.with_memory_space_constraint(x, pltpu.VMEM)


def three_parts(x):
    high = lax.reduce_precision(x, 8, 7)
    middle = lax.reduce_precision(x - high, 8, 7)
    low = x - high - middle
    return jnp.concatenate([high, middle, low], axis=0).astype(jnp.bfloat16)


def rope_tables(offset, rows):
    half = HEAD // 2
    places = jnp.arange(LANES)
    inverse = 10000.0 ** (-(places % half).astype(jnp.float32) / half)
    starts = (offset + QB * jnp.arange(rows // QB)).astype(jnp.float32)
    coarse = starts[:, None] * inverse[None, :]
    sign = np.where(np.arange(LANES) % HEAD < half, -1.0, 1.0)
    exact = np.tile(10000.0 ** (-np.arange(half) / half), 4)
    fine = np.arange(QB)[:, None] * exact[None, :]
    fine = jnp.asarray(np.stack([np.cos(fine), np.sin(fine) * sign]), jnp.float32)
    sine = jnp.sin(coarse)
    return jnp.cos(coarse), jnp.where(places % HEAD < half, -sine, sine), fine


def turned(x, cosine, sine, fine, first_block):
    cosines, sines = [], []
    for block in range(x.shape[0] // QB):
        c, s = cosine[pl.ds(first_block + block, 1), :], sine[pl.ds(first_block + block, 1), :]
        cosines.append(c * fine[0] - s * fine[1])
        sines.append(s * fine[0] + c * fine[1])
    lane = lax.broadcasted_iota(jnp.int32, x.shape, 1)
    half = HEAD // 2
    other = jnp.where(lane % HEAD < half, pltpu.roll(x, LANES - half, 1), pltpu.roll(x, half, 1))
    return x * jnp.concatenate(cosines, axis=0) + other * jnp.concatenate(sines, axis=0)


def project(tokens, gain, own, other, cosine, sine, fine, normed_out, q_out, pool_out, parts, weights):
    core = lax.axis_index("c")
    for place in range(2):

        @pl.when((pl.program_id(0) == 0) & (core == place))
        def _():
            for source, head in ((own, place), (other, 1 - place)):
                weights[head * HEAD : (head + 1) * HEAD] = source[:HEAD]
                weights[LANES + head * HEAD : LANES + (head + 1) * HEAD] = source[HEAD:LANES]
                parts[head * EDGE : (head + 1) * EDGE] = source[LANES:, :LANES]

    values = tokens[...].astype(jnp.float32)
    center = jnp.mean(values, axis=-1, keepdims=True)
    values = values - center
    spread = jnp.mean(values * values, axis=-1, keepdims=True)
    normed = (values * lax.rsqrt(spread + 1e-06) * gain[...]).astype(jnp.bfloat16)
    normed_out[...] = normed
    sums = lax.dot_general(
        normed, weights[...], (((1,), (1,)), ((), ())), preferred_element_type=jnp.float32
    )
    first_block = pl.program_id(0) * (ROWS // QB)
    query = turned(sums[:, :LANES], cosine, sine, fine, first_block)
    here = pl.ds(pl.multiple_of(pl.program_id(0) * ROWS, ROWS), ROWS)
    q_out[here, :] = (query * HEAD ** (-0.5)).astype(jnp.bfloat16)
    pool_out[here, :] = sums[:, LANES:].astype(jnp.bfloat16)


def project_kv(normed, pool, ex, cosine, sine, fine, kv_out, send):
    core, step, rows = lax.axis_index("c"), pl.program_id(0), normed.shape[0]
    sums = jnp.dot(normed[...], ex[...].reshape(-1, LANES), preferred_element_type=jnp.float32)
    lane = lax.broadcasted_iota(jnp.int32, sums.shape, 1)
    kv = jnp.where(lane < HEAD, turned(sums, cosine, sine, fine, step * (rows // QB)), sums)
    kv = kv.astype(jnp.bfloat16)
    kv_out[pl.ds(pl.multiple_of(step * rows, rows), rows), :] = kv

    @pl.when((step == 0) & (core == 1))
    def _():
        send[:QB] = kv[:QB]
        send[QB:] = pool[:EDGE]

    @pl.when((step == pl.num_programs(0) - 1) & (core == 0))
    def _():
        send[:QB] = kv[rows - QB :]
        send[QB:] = pool[pool.shape[0] - EDGE :]


def mix(inner, parts, q, kv, pool, *rest):
    out, kv_wide, pool_wide, both, sems = rest[-5:]
    core, group = lax.axis_index("c"), lax.axis_index("x")
    rows = q.shape[0]
    blocks_total = lax.axis_size(SP) * (rows // QB)
    first_block = lax.axis_index(SP) * (rows // QB)
    first = jnp.sum(parts[:3].astype(jnp.float32), axis=0, keepdims=True)
    second = jnp.sum(parts[EDGE : EDGE + 3].astype(jnp.float32), axis=0, keepdims=True)
    scale = jnp.concatenate([first[:, :HEAD], second[:, :HEAD]], axis=1)
    kv_wide[pl.ds(pl.multiple_of((1 - core) * QB, QB), rows), :] = kv[...]
    pool_wide[EDGE : EDGE + rows, :] = pool[...].astype(jnp.float32)
    if not inner:
        halo = rest[0]
        kv_wide[pl.ds(pl.multiple_of(core * rows, QB), QB), :] = halo[:QB, :]
        edge = halo[QB:, :].astype(jnp.float32)
        pool_wide[:EDGE, :] = edge
        pool_wide[EDGE + rows :, :] = edge
    lane = lax.broadcasted_iota(jnp.int32, (QB, LANES), 1)
    row = lax.broadcasted_iota(jnp.int32, (2 * QB, 3 * QB), 0) % QB
    column = lax.broadcasted_iota(jnp.int32, (2 * QB, 3 * QB), 1)
    near = (column >= row) & (column <= row + 2 * WINDOW)
    upper = lax.broadcasted_iota(jnp.int32, (2 * QB, 1), 0) < QB
    sinks = jnp.where(upper, first[:, HEAD : HEAD + 1], second[:, HEAD : HEAD + 1])
    half = lax.shift_left(1, group)
    copies = []
    for j in range(both.shape[0]):
        i = 1 - core + j if inner else core * (rows // (2 * QB) - 1)
        start = pl.multiple_of(core * QB + 2 * QB * i, QB)
        block = first_block + core + 2 * i
        pair = q[pl.ds(start, QB), :]
        zero = jnp.zeros_like(pair)
        lower_head = jnp.where(lane < HEAD, pair, zero)
        upper_head = jnp.concatenate([pair[:, HEAD:], zero[:, HEAD:]], axis=1)
        queries = jnp.concatenate([lower_head, upper_head], axis=0)
        keys = kv_wide[pl.ds(pl.multiple_of(2 * QB * i, QB), 3 * QB), :]
        scores = lax.dot_general(
            queries, keys, (((1,), (1,)), ((), ())), preferred_element_type=jnp.float32
        )
        least = jnp.where(block == 0, QB, 0)
        limit = jnp.where(block == blocks_total - 1, 2 * QB, 3 * QB)
        valid = near & (column >= least) & (column < limit)
        scores = jnp.where(valid, scores, NEG_BIG)
        top = jnp.maximum(jnp.max(scores, axis=-1, keepdims=True), sinks)
        expo = jnp.where(valid, jnp.exp(scores - top), 0.0)
        total = jnp.sum(expo, axis=-1, keepdims=True) + jnp.exp(sinks - top)
        weights = (expo / total).astype(jnp.bfloat16)
        mixed = jnp.dot(weights, keys, preferred_element_type=jnp.float32)
        attended = jnp.concatenate([mixed[:QB, HEAD:], mixed[QB:, HEAD:]], axis=1)

        near_rows = pool_wide[pl.ds(start, QB + 2 * EDGE), :]
        size = QB + 2 * EDGE
        sums = near_rows + pltpu.roll(near_rows, 1, 0)
        chosen = sums
        for index in range(1, len(POOL_SPANS)):
            step = POOL_SPANS[index] // 4
            sums = pltpu.roll(sums, step, 0) + pltpu.roll(sums, size - step, 0)
            chosen = jnp.where(group == index, sums, chosen)
        position = block * QB + lax.broadcasted_iota(jnp.int32, (QB, 1), 0)
        counted = jnp.minimum(position + half, blocks_total * QB) - jnp.maximum(position - half, 0)
        mean = chosen[EDGE : EDGE + QB] / counted.astype(jnp.float32)
        pooled = (mean - near_rows[EDGE : EDGE + QB]) * scale
        both[j] = jnp.concatenate([attended, pooled], axis=1).astype(jnp.bfloat16)
        for peer in range(out.shape[0]):
            target = out.at[peer, pl.ds(pl.multiple_of(i * QB, QB), QB)]
            copies.append(pltpu.make_async_copy(both.at[j], target, sems.at[j, peer]))
            copies[-1].start()
    for copy in copies:
        copy.wait()


def body(tokens, norm_gain, w_query, w_key, w_value, w_pool_in, sink_logit, pool_scale, w_out):
    rows, depth = tokens.shape
    sp_count = lax.axis_size(SP)
    bf16 = jnp.bfloat16

    key_head = lax.axis_index("x") // (lax.axis_size("x") // (w_key.shape[1] // HEAD))
    key_cols = lax.dynamic_slice_in_dim(w_key, key_head * HEAD, HEAD, 1)
    value_cols = lax.dynamic_slice_in_dim(w_value, key_head * HEAD, HEAD, 1)
    exchanged = from_everyone(jnp.concatenate([key_cols, value_cols], axis=1), SP)
    peers, _ = exchanged.shape[:2]

    out_piece = swapped(w_out.T)

    small = jnp.concatenate([pool_scale, jnp.broadcast_to(sink_logit, (HEAD,))])[None, :]
    small = three_parts(lax.optimization_barrier(small))
    small = jnp.pad(small, ((0, EDGE - 3), (0, depth - LANES)))
    own = jnp.concatenate([w_query.T, w_pool_in.T, small], axis=0)
    other = lax.ppermute(own, "c", [(0, 1), (1, 0)])

    cosine, sine, fine = rope_tables(lax.axis_index(SP) * rows, rows)

    held = pl.BlockSpec(memory_space=pltpu.VMEM)
    whole = lambda *shape: pl.BlockSpec(shape, lambda i: (0,) * len(shape))
    part = lambda *shape: pl.BlockSpec(shape, lambda i: (i,) + (0,) * (len(shape) - 1))
    shaped = lambda *shape: jax.ShapeDtypeStruct(shape, bf16)
    kept = lambda *shape: shaped(*shape) if INTERPRET else pltpu.VMEM(shape, bf16)
    tables = [whole(*cosine.shape)] * 2 + [whole(*fine.shape)]
    normed, query, pool_in, parts = pl.pallas_call(
        project,
        grid=(rows // ROWS,),
        in_specs=[part(ROWS, depth), whole(1, depth)] + [held] * 2 + tables,
        out_specs=[part(ROWS, depth)] + [held] * 3,
        out_shape=[shaped(rows, depth)]
        + [kept(rows, LANES)] * 2
        + [kept(2 * EDGE, LANES)],
        scratch_shapes=[pltpu.VMEM((2 * LANES, depth), bf16)],
        name="project",
        interpret=INTERPRET,
    )(tokens, norm_gain[None, :], on_chip(own), on_chip(other), cosine, sine, fine)
    spread = jnp.broadcast_to(out_piece[None], (peers, *out_piece.shape))
    exchanged, spread, normed = lax.optimization_barrier((exchanged, spread, normed))
    own_cols = lax.all_to_all(spread, SP, 0, 0, tiled=True)
    kv, send = pl.pallas_call(
        project_kv,
        grid=(rows // KV_ROWS,),
        in_specs=[part(KV_ROWS, depth), held, held]
        + tables,
        out_specs=[held, held],
        out_shape=[kept(rows, LANES), kept(QB + EDGE, LANES)],
        name="project_kv",
        interpret=INTERPRET,
    )(normed, on_chip(pool_in), on_chip(exchanged), cosine, sine, fine)

    pairs = [(2 * s, 2 * s + 2) for s in range(sp_count - 1)]
    pairs += [(2 * s + 3, 2 * s + 1) for s in range(sp_count - 1)]
    halo = lax.ppermute(send, SP + ("c",), pairs)
    peers_x = lax.axis_size("x")
    anywhere = pl.BlockSpec(memory_space=pl.ANY)
    local_specs = [held] * 4

    def mixed(inner, *more):
        blocks = rows // (2 * QB) - 1 if inner else 1
        return pl.pallas_call(
            functools.partial(mix, inner),
            grid=(1,),
            in_specs=local_specs + ([] if inner else [held, anywhere]),
            out_specs=anywhere,
            out_shape=shaped(peers_x, rows // 2, 2 * LANES),
            input_output_aliases={} if inner else {5: 0},
            scratch_shapes=[
                pltpu.VMEM((rows + QB, LANES), bf16),
                pltpu.VMEM((rows + 2 * EDGE, LANES), jnp.float32),
                pltpu.VMEM((blocks, QB, 2 * LANES), bf16),
                pltpu.SemaphoreType.DMA((blocks, peers_x)),
            ],
            name="mix_inner" if inner else "mix_outer",
            interpret=INTERPRET,
        )(on_chip(parts), on_chip(query), on_chip(kv), on_chip(pool_in), *more)

    local = mixed(True)
    local = mixed(False, on_chip(halo), local)

    local, own_cols = lax.optimization_barrier((local, own_cols))
    other_cols = lax.ppermute(own_cols, "c", [(0, 1), (1, 0)])
    joined = lax.all_to_all(local, "x", 0, 0, tiled=True)

    def matched(columns):
        columns = columns.reshape(2, peers_x, -1, LANES)
        return jnp.concatenate([columns[0], columns[1]], axis=2)

    core = lax.axis_index("c")
    mine, theirs = matched(own_cols), matched(other_cols)
    columns = jnp.concatenate(
        [jnp.where(core == 0, mine, theirs), jnp.where(core == 0, theirs, mine)], axis=1
    )
    partial_cols = jnp.einsum(
        "ptc,pnc->tn", joined, columns, preferred_element_type=jnp.float32
    ).astype(bf16)
    return lax.all_to_all(partial_cols, "x", split_axis=0, concat_axis=1, tiled=True)


def solution(mesh):
    devices = mesh.devices
    mesh = Mesh(devices.reshape(8, devices.size // 64, 4, 2), SP + TP)
    in_specs = (
        P(SP, None),
        P(),
        P(None, TP),
        P(SP, None),
        P(SP, None),
        P(None, TP),
        P(TP),
        P(TP),
        P(TP, SP),
    )
    out_specs = P(SP + TP, None)
    return jax.shard_map(body, mesh=mesh, in_specs=in_specs, out_specs=out_specs, check_vma=False)
```
